256 devices in a mesh: sp: 64 (over z, y, core), tp: 4 (over x).
Axes of the slice: x: 4, y: 4, z: 8, core: 2. Of those that a mesh axis runs over, the one named last changes fastest.
Arguments:
- residual: bfloat16 [24576, 2048], P(('sp', 'tp')), may hold values from -6 to 6
- query_one: bfloat16 [24576, 512], P('sp', 'tp'), may hold values from -6 to 6
- key_one: bfloat16 [24576, 512], P('sp', 'tp'), may hold values from -6 to 6
- value_one: bfloat16 [24576, 1024], P('sp', 'tp'), may hold values from -6 to 6
- gate_one: bfloat16 [24576, 1024], P('sp', 'tp'), may hold values from -6 to 6
- decay_one: bfloat16 [2, 24576, 512], P(None, 'sp', 'tp'), may hold values from -12 to 12
- norm_one: float32 [128], replicated, may hold values from 0.1 to 1.9
- output_one: bfloat16 [1024, 2048], P('tp'), may hold values from -0.125 to 0.125
- query_two: bfloat16 [24576, 1024], P('sp', 'tp'), may hold values from -6 to 6
- key_two: bfloat16 [24576, 1024], P('sp', 'tp'), may hold values from -6 to 6
- value_two: bfloat16 [24576, 1024], P('sp', 'tp'), may hold values from -6 to 6
- gate_two: bfloat16 [24576, 1024], P('sp', 'tp'), may hold values from -6 to 6
- decay_two: bfloat16 [2, 24576, 1024], P(None, 'sp', 'tp'), may hold values from -12 to 12
- norm_two: float32 [128], replicated, may hold values from 0.1 to 1.9
- output_two: bfloat16 [1024, 2048], P('tp'), may hold values from -0.125 to 0.125
- norm_gain: float32 [2048], replicated, may hold values from 0.1 to 1.9
- expert_ids: int32 [24576, 2], P('sp'), may hold values from 0 to 63, as said below
- group_weight: float32 [24576], P('sp'), may hold values from 0.25 to 1
- pair_weight: float32 [24576, 2], P('sp'), may hold values from 0.05 to 1
- expert_gate: bfloat16 [64, 2048, 1024], P('sp', None, 'tp'), may hold values from -0.125 to 0.125
- expert_up: bfloat16 [64, 2048, 1024], P('sp', None, 'tp'), may hold values from -0.125 to 0.125
- expert_down: bfloat16 [64, 1024, 2048], P('sp', 'tp'), may hold values from -0.1875 to 0.1875
Outputs:
- layer_out: bfloat16 [24576, 2048], P(('sp', 'tp'))
The draws below stay inside these ranges and needn't reach their ends.
Inputs may be any that keep to these rules, and one draw needn't show every extreme that they name: `expert_ids`: each row names two different experts of one group, the group of expert e being e // 16. In each aligned block of 96 rows no expert is named more than 4 times, and one expert, the same in every block, is named exactly 4 times in each block.
All inputs are finite; a program needn't handle non-finite values.
Results may differ from the reference program's by a relative error of at most 0.018.
Values may be sent and summed in bfloat16 or wider, within the bound.
A program may use at most 128 MiB of HBM per device.

```python
import math
from functools import partial
import jax
import jax.numpy as jnp
from jax import lax

D = 2048
HEADS_ONE = 8
KEY_ONE = 64
HEADS_TWO = 8
KEY_TWO = 128
VALUE_W = 128
FF = 1024
BLOCK = 64
GROUPS = 4
TOK_DEV = 384
SEQUENCE_TOKENS = 24576
ROWS_DEV = 96
EXPERTS = 64
EXP_GROUP = 16
CAPACITY = 4
N_TP = 4


def decay_law(key, channels):
    random_keys = jax.random.split(key, 6)
    slow = jax.random.uniform(random_keys[0], (2, 1, channels)) < 0.5
    random_jitter = 0.5 * jax.random.normal(random_keys[1], (2, SEQUENCE_TOKENS, channels))
    channel_factor = jnp.exp(jax.random.uniform(random_keys[2], (2, 1, channels), minval=math.log(0.5), maxval=math.log(1.5)))
    device_factor = jnp.exp(jax.random.uniform(random_keys[3], (2, SEQUENCE_TOKENS // TOK_DEV, 1), minval=math.log(0.5), maxval=math.log(1.5)))
    device_factor = jnp.repeat(device_factor, TOK_DEV, axis=1)
    slow_rate = 0.35 * channel_factor * device_factor / SEQUENCE_TOKENS
    fast_rate = 1.0 / (BLOCK * channel_factor)
    rate = jnp.where(slow, slow_rate, fast_rate)
    smoothed_values = -jnp.log(jnp.expm1(16.0 * rate)) + random_jitter
    spike_position = jax.random.randint(random_keys[4], (2, 2, 1), 0, SEQUENCE_TOKENS)
    retained_entries = jax.random.uniform(random_keys[5], (2, 2, 1), minval=0.5, maxval=0.8)
    spike_value = -jnp.log(jnp.expm1(-16.0 * jnp.log(retained_entries)))
    token_positions = jnp.arange(SEQUENCE_TOKENS, dtype=jnp.int32)[None, None, :]
    match_flags = token_positions == spike_position
    spike_row = jnp.sum(jnp.where(match_flags, spike_value, 0.0), axis=1)
    any_match_found = jnp.any(match_flags, axis=1)
    final_output = jnp.where(any_match_found[:, :, None], spike_row[:, :, None] + 0.1 * random_jitter, smoothed_values)
    return jnp.clip(final_output, -12.0, 12.0).astype(jnp.bfloat16)


def draw_decay_one(key, part):
    return decay_law(jax.random.fold_in(key, 11), HEADS_ONE * KEY_ONE)


def draw_decay_two(key, part):
    return decay_law(jax.random.fold_in(key, 12), HEADS_TWO * KEY_TWO)


def route_block(key, hot):
    order_key, group_key, member_key = jax.random.split(key, 3)
    order = jax.random.permutation(order_key, ROWS_DEV).astype(jnp.int32)
    group_score = jax.random.randint(group_key, (ROWS_DEV, GROUPS), 0, 1 << 20) * GROUPS + jnp.arange(GROUPS, dtype=jnp.int32)
    member_score = jax.random.randint(member_key, (ROWS_DEV, EXPERTS), 0, 1 << 20) * EXPERTS + jnp.arange(EXPERTS, dtype=jnp.int32)
    labels = jnp.arange(EXPERTS, dtype=jnp.int32)

    def place_row(counts, step):
        row = order[step]
        forced = step < CAPACITY
        free = counts < CAPACITY
        usable = jnp.sum(free.reshape(GROUPS, EXP_GROUP).astype(jnp.int32), axis=1) >= 2
        picked_group = jnp.argmax(jnp.where(usable, group_score[row], -1)).astype(jnp.int32)
        chosen_group = jnp.where(forced, hot // EXP_GROUP, picked_group)
        allowed = free & (labels // EXP_GROUP == chosen_group)
        scored = jnp.where(allowed, member_score[row], -1)
        first = jnp.where(forced, hot, jnp.argmax(scored).astype(jnp.int32))
        second = jnp.argmax(jnp.where(labels == first, -1, scored)).astype(jnp.int32)
        counts = counts + (labels == first).astype(jnp.int32) + (labels == second).astype(jnp.int32)
        return (counts, (row, first, second))
    _, (rows, firsts, seconds) = lax.scan(place_row, jnp.zeros((EXPERTS,), jnp.int32), jnp.arange(ROWS_DEV, dtype=jnp.int32))
    return jnp.zeros((ROWS_DEV, 2), jnp.int32).at[rows].set(jnp.stack([firsts, seconds], axis=1))


def draw_expert_ids(key, part):
    hot_key, block_key = jax.random.split(jax.random.fold_in(key, 21))
    hot = jax.random.randint(hot_key, (), 0, EXPERTS).astype(jnp.int32)
    random_keys = jax.random.split(block_key, SEQUENCE_TOKENS // ROWS_DEV)
    blocks = jax.vmap(partial(route_block, hot=hot))(random_keys)
    return blocks.reshape(SEQUENCE_TOKENS, 2)


def levels(key, shape, shards, low, high):
    level = 1.0
    for axis_at, shards_of in shards:
        draws = jax.random.uniform(jax.random.fold_in(jax.random.fold_in(key, 6), axis_at), (shards_of,), jnp.float32, low / len(shards), high / len(shards))
        level = level * jnp.repeat(jnp.exp(draws), shape[axis_at] // shards_of).reshape((-1,) + (1,) * (len(shape) - 1 - axis_at))
    return level


def bell_draw(rng, shape, spread, most, shards=(), kind=jnp.bfloat16):
    values = spread * jax.random.normal(rng, shape, jnp.float32)
    if shards:
        values = values * levels(rng, shape, shards, -0.22, 0.18)
    return jnp.clip(values, -most, most).astype(kind)


def setup_inputs(seed: int = 0) -> dict:
    streams_of = jax.random.split(jax.random.key(seed), 23)
    return {
        "residual": bell_draw(streams_of[0], (SEQUENCE_TOKENS, D), 1.0, 6.0, ((0, 256),)),
        "query_one": bell_draw(streams_of[1], (SEQUENCE_TOKENS, HEADS_ONE * KEY_ONE), 1.0, 6.0, ((0, 64), (1, 4))),
        "key_one": bell_draw(streams_of[2], (SEQUENCE_TOKENS, HEADS_ONE * KEY_ONE), 1.0, 6.0, ((0, 64), (1, 4))),
        "value_one": bell_draw(streams_of[3], (SEQUENCE_TOKENS, HEADS_ONE * VALUE_W), 1.0, 6.0, ((0, 64), (1, 4))),
        "gate_one": bell_draw(streams_of[4], (SEQUENCE_TOKENS, HEADS_ONE * VALUE_W), 1.0, 6.0, ((0, 64), (1, 4))),
        "decay_one": draw_decay_one(jax.random.fold_in(streams_of[22], 71), 0),
        "norm_one": jnp.clip(1.0 + 0.18 * jax.random.normal(streams_of[6], (VALUE_W,), jnp.float32), 0.1, 1.9),
        "output_one": bell_draw(streams_of[7], (HEADS_ONE * VALUE_W, D), ((HEADS_ONE + HEADS_TWO) * VALUE_W) ** -0.5, 0.125, ((0, 4),)),
        "query_two": bell_draw(streams_of[8], (SEQUENCE_TOKENS, HEADS_TWO * KEY_TWO), 1.0, 6.0, ((0, 64), (1, 4))),
        "key_two": bell_draw(streams_of[9], (SEQUENCE_TOKENS, HEADS_TWO * KEY_TWO), 1.0, 6.0, ((0, 64), (1, 4))),
        "value_two": bell_draw(streams_of[10], (SEQUENCE_TOKENS, HEADS_TWO * VALUE_W), 1.0, 6.0, ((0, 64), (1, 4))),
        "gate_two": bell_draw(streams_of[11], (SEQUENCE_TOKENS, HEADS_TWO * VALUE_W), 1.0, 6.0, ((0, 64), (1, 4))),
        "decay_two": draw_decay_two(jax.random.fold_in(streams_of[22], 71), 0),
        "norm_two": jnp.clip(1.0 + 0.18 * jax.random.normal(streams_of[13], (VALUE_W,), jnp.float32), 0.1, 1.9),
        "output_two": bell_draw(streams_of[14], (HEADS_TWO * VALUE_W, D), ((HEADS_ONE + HEADS_TWO) * VALUE_W) ** -0.5, 0.125, ((0, 4),)),
        "norm_gain": jnp.clip(1.0 + 0.18 * jax.random.normal(streams_of[15], (D,), jnp.float32), 0.1, 1.9),
        "expert_ids": draw_expert_ids(jax.random.fold_in(streams_of[22], 71), 0),
        "group_weight": jnp.clip(jnp.exp(math.log(1.0) - 1.3862944 * jax.random.uniform(streams_of[17], (SEQUENCE_TOKENS,), jnp.float32) ** levels(streams_of[17], (SEQUENCE_TOKENS,), ((0, 64),), -0.2, 0.2)), 0.25, 1.0),
        "pair_weight": jnp.clip(jnp.exp(math.log(1.0) - 2.9957323 * jax.random.uniform(streams_of[18], (SEQUENCE_TOKENS, 2), jnp.float32) ** levels(streams_of[18], (SEQUENCE_TOKENS, 2), ((0, 64),), -0.2, 0.2)), 0.05, 1.0),
        "expert_gate": bell_draw(streams_of[19], (EXPERTS, D, FF), D ** -0.5, 0.125, ((0, 64), (2, 4))),
        "expert_up": bell_draw(streams_of[20], (EXPERTS, D, FF), D ** -0.5, 0.125, ((0, 64), (2, 4))),
        "expert_down": bell_draw(streams_of[21], (EXPERTS, FF, D), FF ** -0.5, 0.1875, ((0, 64), (1, 4))),
    }


HIGH = lax.Precision.HIGHEST
TAU = 16.0
EPS = 1e-06

def advance(state_now, step_input):
    fade_rate, extra_term = step_input
    return (fade_rate[..., None] * state_now + extra_term, state_now)

def block_pass(queries, key_rows, values, rates):
    length, heads, width = queries.shape
    blocks = length // BLOCK
    shaped = (blocks, BLOCK, heads, width)
    cumul = jnp.cumsum(rates.reshape(shaped), axis=1)
    block_end = cumul[:, -1]
    key_blocks = key_rows.reshape(shaped)
    value_blocks = values.reshape(blocks, BLOCK, heads, values.shape[-1])
    query_dec = queries.reshape(shaped) * jnp.exp(cumul)
    query_low = query_dec.astype(jnp.bfloat16)
    key_dec = (key_blocks * jnp.exp(-cumul)).astype(jnp.bfloat16)
    key_end = (key_blocks * jnp.exp(block_end[:, None] - cumul)).astype(jnp.bfloat16)
    lower_mask = jnp.tril(jnp.ones((BLOCK, BLOCK), jnp.float32))
    scores = jnp.einsum('nthd,nshd->nhts', query_low, key_dec, preferred_element_type=jnp.float32) * lower_mask
    scores = scores.astype(jnp.bfloat16)
    inner_part = jnp.einsum('nhts,nshe->nthe', scores, value_blocks, preferred_element_type=jnp.float32)
    added = jnp.einsum('nshd,nshe->nhde', key_end, value_blocks, preferred_element_type=jnp.float32)
    empty = jnp.zeros((heads, width, values.shape[-1]), jnp.float32)
    state_out, before = lax.scan(advance, empty, (jnp.exp(block_end), added))
    outer_part = jnp.einsum('nthd,nhde->nthe', query_dec, before, precision=HIGH)
    return (inner_part + outer_part).reshape(length, heads, values.shape[-1])

def group_mix(query, key_in, value, gate, decay, gain, width):
    heads = query.shape[1] // width
    queries = query.astype(jnp.float32).reshape(SEQUENCE_TOKENS, heads, width) * width ** (-0.5)
    key_rows = key_in.astype(jnp.float32).reshape(SEQUENCE_TOKENS, heads, width)
    values = value.reshape(SEQUENCE_TOKENS, heads, VALUE_W)
    rates = jax.nn.log_sigmoid(decay.astype(jnp.float32)) / TAU
    ahead = block_pass(queries, key_rows, values, rates[0].reshape(SEQUENCE_TOKENS, heads, width))
    behind = block_pass(jnp.flip(queries, 0), jnp.flip(key_rows, 0), jnp.flip(values, 0), jnp.flip(rates[1], 0).reshape(SEQUENCE_TOKENS, heads, width))
    total = ahead + jnp.flip(behind, 0)
    scale = lax.rsqrt(lax.optimization_barrier(jnp.mean(total * total, axis=-1, keepdims=True)) + EPS)
    normed = (total * scale * gain).reshape(SEQUENCE_TOKENS, heads * VALUE_W)
    return (normed * jax.nn.silu(gate.astype(jnp.float32))).astype(jnp.bfloat16)

def rounded(term):
    return lax.optimization_barrier(term.astype(jnp.bfloat16)).astype(jnp.float32)

def slot_table(routes, capacity, experts):
    flat = routes.reshape(-1)
    count = flat.shape[0]
    onehot = (flat[:, None] == jnp.arange(experts, dtype=jnp.int32)[None, :]).astype(jnp.int32)
    place = lax.optimization_barrier(jnp.sum((jnp.cumsum(onehot, axis=0) - onehot) * onehot, axis=1)).astype(jnp.int32)
    table = jnp.full((experts, capacity), count, jnp.int32).at[flat, place].set(jnp.arange(count, dtype=jnp.int32))
    return (table, place)

def reference(residual, query_one, key_one, value_one, gate_one, decay_one, norm_one, output_one, query_two, key_two, value_two, gate_two, decay_two, norm_two, output_two, norm_gain, expert_ids, group_weight, pair_weight, expert_gate, expert_up, expert_down):
    mixed_one = group_mix(query_one, key_one, value_one, gate_one, decay_one, norm_one, KEY_ONE)
    mixed_two = group_mix(query_two, key_two, value_two, gate_two, decay_two, norm_two, KEY_TWO)
    span_one = mixed_one.shape[1] // N_TP
    span_two = mixed_two.shape[1] // N_TP
    projected = jnp.zeros((SEQUENCE_TOKENS, D), jnp.float32)
    for part in range(N_TP):
        term = jnp.dot(mixed_one[:, part * span_one:(part + 1) * span_one], output_one[part * span_one:(part + 1) * span_one], preferred_element_type=jnp.float32)
        term = term + jnp.dot(mixed_two[:, part * span_two:(part + 1) * span_two], output_two[part * span_two:(part + 1) * span_two], preferred_element_type=jnp.float32)
        projected = projected + rounded(term)
    stream = (residual.astype(jnp.float32) + rounded(projected)).astype(jnp.bfloat16)
    wide = stream.astype(jnp.float32)
    normed = (wide * lax.rsqrt(lax.optimization_barrier(jnp.mean(wide * wide, axis=-1, keepdims=True)) + EPS) * norm_gain).astype(jnp.bfloat16)
    weights = group_weight[:, None] * pair_weight / lax.optimization_barrier(jnp.sum(pair_weight, axis=1, keepdims=True))
    blocks = SEQUENCE_TOKENS // ROWS_DEV
    tables, places = jax.vmap(partial(slot_table, capacity=CAPACITY, experts=EXPERTS))(expert_ids.reshape(blocks, ROWS_DEV, 2))
    offsets = (jnp.arange(blocks, dtype=jnp.int32) * (2 * ROWS_DEV))[:, None, None]
    assigned = jnp.where(tables == 2 * ROWS_DEV, 2 * SEQUENCE_TOKENS, tables + offsets).astype(jnp.int32)
    assigned = jnp.transpose(assigned, (1, 0, 2)).reshape(EXPERTS, blocks * CAPACITY)
    padded = jnp.concatenate([normed, jnp.zeros((1, D), jnp.bfloat16)], axis=0)
    route_weight = jnp.concatenate([weights.reshape(-1), jnp.zeros((1,), jnp.float32)])
    span = FF // N_TP

    def expert_pass(total, step_input):
        index, weight_gate, weight_up, weight_down = step_input
        token = index // 2
        rows = padded[token]
        gate_part = jnp.dot(rows, weight_gate, preferred_element_type=jnp.float32)
        up_part = jnp.dot(rows, weight_up, preferred_element_type=jnp.float32)
        hidden = (jax.nn.silu(gate_part) * up_part).astype(jnp.bfloat16)
        summed = jnp.zeros((rows.shape[0], D), jnp.float32)
        for part in range(N_TP):
            summed = summed + rounded(jnp.dot(hidden[:, part * span:(part + 1) * span], weight_down[part * span:(part + 1) * span], preferred_element_type=jnp.float32))
        final_output = rounded(summed)
        return (total.at[token].add(route_weight[index][:, None] * final_output), None)
    total, _ = lax.scan(expert_pass, jnp.zeros((SEQUENCE_TOKENS + 1, D), jnp.float32), (assigned, expert_gate, expert_up, expert_down))
    return (stream.astype(jnp.float32) + total[:SEQUENCE_TOKENS]).astype(jnp.bfloat16)
```

```python
import functools

import jax
import jax.numpy as jnp
from jax import lax
from jax.experimental import pallas as pl
from jax.experimental.pallas import tpu as pltpu
from jax.sharding import Mesh
from jax.sharding import PartitionSpec as P

D = 2048
BLOCK = 64
NB = 6
KEYS = 384
SP = ("sp_0", "sp_1", "sp_2")
SP_TP = ("sp_0", "sp_1", "sp_2", "tp")
EPS = 1e-06
F32 = jnp.float32
BF16 = jnp.bfloat16


def place():
    return tuple(lax.axis_index(a) for a in SP_TP)


def dev(z, y, c, x):
    return {"sp_0": z, "sp_1": y, "sp_2": c, "tp": x}


def remote(src, dst, ssem, rsem, device):
    return pltpu.make_async_remote_copy(
        src_ref=src,
        dst_ref=dst,
        send_sem=ssem,
        recv_sem=rsem,
        device_id=device,
        device_id_type=pl.DeviceIdType.MESH,
    )


def greet(barrier, device):
    pl.semaphore_signal(barrier, inc=1, device_id=device, device_id_type=pl.DeviceIdType.MESH)


def nn(a, b):
    return lax.dot_general(a, b, (((1,), (0,)), ((), ())), preferred_element_type=F32)


def nt(a, b):
    return lax.dot_general(a, b, (((1,), (1,)), ((), ())), preferred_element_type=F32)


def tn(a, b):
    return lax.dot_general(a, b, (((0,), (0,)), ((), ())), preferred_element_type=F32)


def iota2(shape, dim):
    return lax.broadcasted_iota(jnp.int32, shape, dim)


def halves(row):
    hi = row.astype(BF16)
    lo = (row - hi.astype(F32)).astype(BF16)
    return hi, lo


def decay_tile(fwd, bwd):
    fh, fl = halves(fwd)
    bh, bl = halves(bwd)
    full = lambda r: jnp.broadcast_to(r.astype(F32), (4, KEYS))
    return jnp.concatenate([full(fh), full(fl), full(bh), full(bl)], axis=0).astype(BF16)


def mixer_kernel(
    q1, k1, v1, g1, d1, n1, q2, k2, v2, g2, d2, n2, ng,
    res_h, ow1_h, ow2_h, eg_h, eu_h, ed_h,
    stream_o, normed_o, pg_o, pu_o, pd_o,
    ow_v, res_v, qd_s, kd_s, add_s, dec_s, acc,
    s1, r1, pre_s, prd_s, s2, r2, s3, r3, mixed, pbuf, prec,
    lsem, wsend, wrecv, xsem, rsem, dsend, drecv,
):
    z, y, c, x = place()
    p = y * 2 + c
    sgn = (1 - 2 * (x % 2)) * (1 - 2 * c)
    xp = (x + sgn + 4) % 4

    loads = [
        pltpu.make_async_copy(ow1_h, ow_v.at[pl.ds(0, 256)], lsem.at[0]),
        pltpu.make_async_copy(ow2_h, ow_v.at[pl.ds(256, 256)], lsem.at[1]),
        pltpu.make_async_copy(res_h, res_v, lsem.at[2]),
    ]
    for cp in loads:
        cp.start()

    barrier = pltpu.get_barrier_semaphore()
    for o in range(1, 8):
        t = (p + o) % 8
        greet(barrier, dev(z, t // 2, t % 2, x))
        greet(barrier, dev((z + o) % 8, y, c, x))
    for o in range(1, 4):
        greet(barrier, dev(z, y, c, (x + o) % 4))
    pl.semaphore_wait(barrier, 17)

    wcopies = [
        remote(src, dst, wsend.at[i], wrecv.at[i], dev(z, y, c, xp))
        for i, (src, dst) in enumerate(((eg_h, pg_o), (eu_h, pu_o), (ed_h, pd_o)))
    ]
    for cp in wcopies:
        cp.start()

    row = iota2((BLOCK, BLOCK), 0)
    col = iota2((BLOCK, BLOCK), 1)
    lower, upper = row >= col, row <= col
    tri = (jnp.where(lower, 1.0, 0.0).astype(BF16), jnp.where(upper, 1.0, 0.0).astype(BF16))
    scale = jnp.where(iota2((1, KEYS), 1) < 128, 64.0 ** -0.5, 128.0 ** -0.5)
    head0 = iota2((1, 128), 1) < 64

    def prepare(way, n):
        rows = pl.ds(n * BLOCK, BLOCK)
        d = jnp.concatenate([d1[way, rows, :], d2[way, rows, :]], axis=1).astype(F32)
        rate = (jnp.minimum(d, 0.0) - jnp.log1p(jnp.exp(-jnp.abs(d)))) * (1.0 / 16.0)
        hi = rate.astype(BF16)
        rest = rate - hi.astype(F32)
        mid = rest.astype(BF16)
        low = (rest - mid.astype(F32)).astype(BF16)
        cum = nn(tri[way], hi) + nn(tri[way], mid) + nn(tri[way], low)
        end = cum[BLOCK - 1 :, :] if way == 0 else cum[0:1, :]
        fade = jnp.exp(end)
        q = jnp.concatenate([q1[rows, :], q2[rows, :]], axis=1).astype(F32)
        k = jnp.concatenate([k1[rows, :], k2[rows, :]], axis=1).astype(F32)
        kd = k * jnp.exp(-cum)
        kr = (kd * fade).astype(BF16)
        qd_s[way, rows, :] = (q * scale * jnp.exp(cum)).astype(BF16)
        kd_s[way, rows, :] = kd.astype(BF16)
        va, vb = v1[rows, 0:128], v1[rows, 128:256]
        vc, vd = v2[rows, 0:128], v2[rows, 128:256]
        one = jnp.where(head0, tn(va, kr[:, 0:128]), tn(vb, kr[:, 0:128]))
        added = jnp.concatenate([one, tn(vc, kr[:, 128:256]), tn(vd, kr[:, 256:384])], axis=1)
        add_s[way, n] = added
        dec_s[way, n] = jnp.broadcast_to(fade, (8, KEYS))

    for n in range(NB):
        prepare(0, n)
        prepare(1, n)

    totals, fades = [], []
    for way in range(2):
        order = range(NB) if way == 0 else range(NB - 1, -1, -1)
        run, fade = None, None
        for n in order:
            f = dec_s[way, n][0:1]
            run = add_s[way, n] if run is None else run * f + add_s[way, n]
            fade = f if fade is None else fade * f
        totals.append(run.astype(BF16))
        fades.append(fade)
    tile = decay_tile(fades[0], fades[1])
    for j in range(8):
        s1[j, 0:16, :] = totals[0][16 * j : 16 * j + 16]
        s1[j, 16:32, :] = totals[1][16 * j : 16 * j + 16]
        s1[j, 32:48, :] = tile
    r1[p] = s1[p]
    for o in range(1, 8):
        t = (p + o) % 8
        remote(s1.at[t], r1.at[p], xsem.at[0], rsem.at[0], dev(z, t // 2, t % 2, x)).start()

    def inner(n):
        rows = pl.ds(n * BLOCK, BLOCK)
        qf, qb = qd_s[0, rows, :], qd_s[1, rows, :]
        kf, kb = kd_s[0, rows, :], kd_s[1, rows, :]
        zero = jnp.zeros((), BF16)
        spans = []
        for h in range(2):
            m = head0 if h == 0 else jnp.logical_not(head0)
            spans.append(
                (jnp.where(m, qf[:, 0:128], zero), kf[:, 0:128],
                 jnp.where(m, qb[:, 0:128], zero), kb[:, 0:128], v1[rows, 128 * h : 128 * h + 128])
            )
        for h in range(2):
            at = slice(128 + 128 * h, 256 + 128 * h)
            spans.append((qf[:, at], kf[:, at], qb[:, at], kb[:, at], v2[rows, 128 * h : 128 * h + 128]))
        for h, (a, b, aa, bb, v) in enumerate(spans):
            s = jnp.where(lower, nt(a, b), 0.0) + jnp.where(upper, nt(aa, bb), 0.0)
            acc[rows, 128 * h : 128 * h + 128] = nn(s.astype(BF16), v)

    for n in range(3):
        inner(n)

    whole7 = lambda ref: ref.at[pl.ds(0, 7)]
    other = dev(z, y, 1 - c, x)
    batch1 = remote(whole7(s1), whole7(r1), xsem.at[0], rsem.at[0], other)
    batch1.wait_recv()

    def unpack(ref, i):
        s = ref[i].astype(F32)
        return s[0:16], s[16:32], s[32:33] + s[36:37], s[40:41] + s[44:45]

    parts = [unpack(r1, i) for i in range(8)]
    run, fade = jnp.zeros((16, KEYS), F32), jnp.ones((1, KEYS), F32)
    for i in range(8):
        pre_s[0, i] = run
        prd_s[0, i] = jnp.broadcast_to(fade, (8, KEYS))
        run = run * parts[i][2] + parts[i][0]
        fade = fade * parts[i][2]
    back, bade = jnp.zeros((16, KEYS), F32), jnp.ones((1, KEYS), F32)
    for i in range(7, -1, -1):
        pre_s[1, i] = back
        prd_s[1, i] = jnp.broadcast_to(bade, (8, KEYS))
        back = back * parts[i][3] + parts[i][1]
        bade = bade * parts[i][3]
    s2[0:16, :] = run.astype(BF16)
    s2[16:32, :] = back.astype(BF16)
    s2[32:48, :] = decay_tile(fade, bade)
    r2[z] = s2[...]
    for o in (4, 3, 5, 2, 6, 1, 7):
        remote(s2, r2.at[z], xsem.at[1], rsem.at[1], dev((z + o) % 8, y, c, x)).start()

    for n in range(3, NB):
        inner(n)

    batch2 = remote(whole7(r2), whole7(r2), xsem.at[1], rsem.at[1], other)
    batch2.wait_recv()
    parts = [unpack(r2, i) for i in range(8)]
    run = jnp.zeros((16, KEYS), F32)
    back = jnp.zeros((16, KEYS), F32)
    for i in range(8):
        run = jnp.where(i < z, run * parts[i][2] + parts[i][0], run)
    for i in range(7, -1, -1):
        back = jnp.where(i > z, back * parts[i][3] + parts[i][1], back)
    for j in range(8):
        s3[j, 0:16, :] = (pre_s[0, j] + prd_s[0, j][0:1] * run).astype(BF16)
        s3[j, 16:32, :] = (pre_s[1, j] + prd_s[1, j][0:1] * back).astype(BF16)
    r3[p] = s3[p]
    for o in range(1, 8):
        t = (p + o) % 8
        remote(s3.at[t], r3.at[p], xsem.at[2], rsem.at[2], dev(z, t // 2, t % 2, x)).start()
    batch3 = remote(whole7(s3), whole7(r3), xsem.at[2], rsem.at[2], other)
    batch3.wait_recv()

    states = [
        jnp.concatenate([r3[j, 16 * w : 16 * w + 16, :] for j in range(8)], axis=0).astype(F32)
        for w in range(2)
    ]
    zero = jnp.zeros((), BF16)
    for i in range(NB):
        for way, n in ((0, i), (1, NB - 1 - i)):
            rows = pl.ds(n * BLOCK, BLOCK)
            low = states[way].astype(BF16)
            qd = qd_s[way, rows, :]
            first = qd[:, 0:128]
            outs = [
                nt(jnp.where(head0, first, zero), low[:, 0:128]),
                nt(jnp.where(head0, zero, first), low[:, 0:128]),
                nt(qd[:, 128:256], low[:, 128:256]),
                nt(qd[:, 256:384], low[:, 256:384]),
            ]
            acc[rows, :] += jnp.concatenate(outs, axis=1)
            if i < NB - 1:
                states[way] = states[way] * dec_s[way, n][0:1] + add_s[way, n]

    for n in range(NB):
        rows = pl.ds(n * BLOCK, BLOCK)
        for h in range(4):
            gate_ref, gain = (g1, n1) if h < 2 else (g2, n2)
            at = 128 * (h % 2)
            t = acc[rows, 128 * h : 128 * h + 128]
            g = gate_ref[rows, at : at + 128].astype(F32)
            ms = jnp.mean(t * t, axis=1, keepdims=True)
            out = t * lax.rsqrt(ms + EPS) * gain[...] * (g / (1.0 + jnp.exp(-g)))
            mixed[rows, 128 * h : 128 * h + 128] = out.astype(BF16)

    for cp in loads:
        cp.wait()
    for o in (2, 1, 3, 0):
        t = (x + o) % 4
        rows = mixed[pl.ds(pl.multiple_of(t * 96, 96), 96), :]
        for q in range(4):
            at = slice(512 * q, 512 * q + 512)
            pbuf[o, :, at] = nn(rows, ow_v[:, at]).astype(BF16)
        if o:
            remote(pbuf.at[o], prec.at[o], dsend.at[o], drecv.at[o], dev(z, y, c, t)).start()

    total = pbuf[0].astype(F32)
    for o in (1, 3, 2):
        remote(pbuf.at[o], prec.at[o], dsend.at[o], drecv.at[o], other).wait_recv()
        total = total + prec[o].astype(F32)
    stream = (res_v[...].astype(F32) + total.astype(BF16).astype(F32)).astype(BF16)
    stream_o[...] = stream
    wide = stream.astype(F32)
    ms = jnp.mean(wide * wide, axis=1, keepdims=True)
    normed_o[...] = (wide * lax.rsqrt(ms + EPS) * ng[...]).astype(BF16)

    batch1.wait_send()
    batch2.wait_send()
    batch3.wait_send()
    for o in (1, 2, 3):
        remote(pbuf.at[o], prec.at[o], dsend.at[o], drecv.at[o], other).wait_send()
    for cp in wcopies:
        cp.wait()


def mixer(q1, k1, v1, g1, d1, n1, q2, k2, v2, g2, d2, n2, ng, res, ow1, ow2, eg, eu, ed):
    vm = pl.BlockSpec(memory_space=pltpu.VMEM)
    hbm = pl.BlockSpec(memory_space=pl.ANY)
    sd = jax.ShapeDtypeStruct
    return pl.pallas_call(
        mixer_kernel,
        name="mixer",
        out_shape=(
            sd((96, D), BF16), sd((96, D), BF16),
            sd(eg.shape, BF16), sd(eu.shape, BF16), sd(ed.shape, BF16),
        ),
        in_specs=[vm] * 13 + [hbm] * 6,
        out_specs=(vm, vm, hbm, hbm, hbm),
        scratch_shapes=[
            pltpu.VMEM((512, D), BF16), pltpu.VMEM((96, D), BF16),
            pltpu.VMEM((2, 384, KEYS), BF16), pltpu.VMEM((2, 384, KEYS), BF16),
            pltpu.VMEM((2, NB, 128, KEYS), F32), pltpu.VMEM((2, NB, 8, KEYS), F32),
            pltpu.VMEM((384, 512), F32),
            pltpu.VMEM((8, 48, KEYS), BF16), pltpu.VMEM((8, 48, KEYS), BF16),
            pltpu.VMEM((2, 8, 16, KEYS), F32), pltpu.VMEM((2, 8, 8, KEYS), F32),
            pltpu.VMEM((48, KEYS), BF16), pltpu.VMEM((8, 48, KEYS), BF16),
            pltpu.VMEM((8, 32, KEYS), BF16), pltpu.VMEM((8, 32, KEYS), BF16),
            pltpu.VMEM((384, 512), BF16), pltpu.VMEM((4, 96, D), BF16), pltpu.VMEM((4, 96, D), BF16),
            pltpu.SemaphoreType.DMA((3,)), pltpu.SemaphoreType.DMA((3,)), pltpu.SemaphoreType.DMA((3,)),
            pltpu.SemaphoreType.DMA((3,)), pltpu.SemaphoreType.DMA((3,)),
            pltpu.SemaphoreType.DMA((4,)), pltpu.SemaphoreType.DMA((4,)),
        ],
        compiler_params=pltpu.CompilerParams(
            collective_id=0, has_side_effects=True, vmem_limit_bytes=48 * 1024 * 1024
        ),
    )(q1, k1, v1, g1, d1, n1, q2, k2, v2, g2, d2, n2, ng, res, ow1, ow2, eg, eu, ed)


def moe_kernel(
    ids, gw, pw, normed, stream, wg_h, wu_h, wd_h, pg_h, pu_h, pd_h,
    out_o,
    wg, wu, wd, send, recv, xb, hid, yown, ypart, yrecv, ret, bk, bb,
    lsem, ssem, rsem, fsend, frecv, psend, precv, bsend, brecv,
):
    z, y, c, x = place()
    me = (z * 4 + y) * 2 + c
    sgn = (1 - 2 * (x % 2)) * (1 - 2 * c)
    xo = (x - sgn + 4) % 4
    facing = dev(z, y, c, xo)

    loads = []
    for i, (src, dst) in enumerate(
        ((wg_h, wg.at[0]), (wu_h, wu.at[0]), (wd_h, wd.at[0]), (pg_h, wg.at[1]), (pu_h, wu.at[1]), (pd_h, wd.at[1]))
    ):
        loads.append(pltpu.make_async_copy(src, dst, lsem.at[i]))
        loads[-1].start()

    def target(o):
        t = (me + o) % 64
        return t, dev(t // 8, (t // 2) % 4, t % 2, x)

    barrier = pltpu.get_barrier_semaphore()

    @pl.loop(1, 64)
    def _(o):
        greet(barrier, target(o)[1])

    greet(barrier, facing)

    own = ids[pl.ds(pl.multiple_of(x * 96, 96), 96), :]
    gate = gw[pl.ds(pl.multiple_of(x * 96, 96), 96), :]
    pair = pw[pl.ds(pl.multiple_of(x * 96, 96), 96), :]
    inv = gate / (pair[:, 0:1] + pair[:, 1:2])
    experts = iota2((96, 64), 1)
    slots = iota2((96, 256), 1).astype(F32)
    m = [jnp.where(own[:, k : k + 1] == experts, 1.0, 0.0) for k in range(2)]
    before = jnp.where(iota2((96, 96), 0) > iota2((96, 96), 1), 1.0, 0.0).astype(BF16)
    count = nn(before, (m[0] + m[1]).astype(BF16))
    picks = []
    for k in range(2):
        at = jnp.sum(count * m[k], axis=1, keepdims=True) + 4.0 * own[:, k : k + 1].astype(F32)
        picks.append(jnp.where(at == slots, 1.0, 0.0))
    select = (picks[0] + picks[1]).astype(BF16)
    weigh = picks[0] * (inv * pair[:, 0:1]) + picks[1] * (inv * pair[:, 1:2])
    weigh_hi, weigh_lo = halves(weigh)

    def scatter_rows(dst, first, rows, at):
        for e in range(rows.shape[0] // 4):
            dst[first + e, :, at] = rows[4 * e : 4 * e + 4, :]

    for q in range(4):
        at = slice(512 * q, 512 * q + 512)
        scatter_rows(send, 0, tn(select, normed[:, at]).astype(BF16), at)

    pl.semaphore_wait(barrier, 64)
    recv[me] = send[me]

    @pl.loop(1, 64)
    def _(o):
        t, device = target(o)
        remote(send.at[t], recv.at[me], ssem.at[0], rsem.at[z], device).start()

    for i, dz in enumerate((0, 1, 7, 2, 6, 3, 5, 4)):
        zs = (z + dz) % 8
        n = 7 if dz == 0 else 8
        remote(send.at[pl.ds(0, n)], recv.at[pl.ds(0, n)], ssem.at[0], rsem.at[zs], facing).wait_recv()
        rows = jnp.concatenate([recv[zs * 8 + j] for j in range(8)], axis=0)
        at = pl.multiple_of(zs * 32, 32)
        xb[pl.ds(at, 32), :] = rows
        remote(
            xb.at[pl.ds(at, 32)], xb.at[pl.ds(pl.multiple_of(256 + at, 32), 32)],
            fsend.at[zs], frecv.at[zs], facing,
        ).start()

    for cp in loads:
        cp.wait()

    def up(first, n):
        rows = xb[first : first + n, :]
        for s in range(2):
            a = nn(rows, wg[s])
            b = nn(rows, wu[s])
            hid[first : first + n, 256 * s : 256 * s + 256] = (a / (1.0 + jnp.exp(-a)) * b).astype(BF16)

    def down(first, n, store):
        for q in range(4):
            at = slice(512 * q, 512 * q + 512)
            h = hid[first : first + n, :]
            store(at, nn(h[:, 0:256], wd[0, :, at]) + nn(h[:, 256:512], wd[1, :, at]))

    up(0, 256)

    def keep(at, val):
        yown[:, at] = val

    down(0, 256, keep)

    HALF = 128
    for part in range(2):
        for i in range(4):
            zs = 4 * part + i
            remote(
                xb.at[pl.ds(32 * zs, 32)], xb.at[pl.ds(256 + 32 * zs, 32)], fsend.at[zs], frecv.at[zs], facing
            ).wait_recv()
        first = 256 + HALF * part
        up(first, HALF)

        def keep_part(at, val):
            ypart[HALF * part : HALF * part + HALF, at] = val.astype(BF16)

        down(first, HALF, keep_part)
        span = pl.ds(HALF * part, HALF)
        remote(ypart.at[span], yrecv.at[span], psend.at[part], precv.at[part], facing).start()

    for part in range(2):
        span = pl.ds(HALF * part, HALF)
        remote(ypart.at[span], yrecv.at[span], psend.at[part], precv.at[part], facing).wait_recv()
        for q in range(4):
            at = slice(512 * q, 512 * q + 512)
            val = yown[HALF * part : HALF * part + HALF, at] + yrecv[HALF * part : HALF * part + HALF, at].astype(F32)
            scatter_rows(ret, 32 * part, val.astype(BF16), at)

    bk[me] = ret[me]

    @pl.loop(1, 64)
    def _(o):
        t, device = target(o)
        remote(ret.at[t], bk.at[me], bsend.at[0], brecv.at[0], device).start()

    remote(ret.at[pl.ds(0, 63)], bk.at[pl.ds(0, 63)], bsend.at[0], brecv.at[0], facing).wait_recv()
    for i in range(8):
        bb[32 * i : 32 * i + 32, :] = jnp.concatenate([bk[8 * i + j] for j in range(8)], axis=0)
    for q in range(4):
        at = slice(512 * q, 512 * q + 512)
        part = nn(weigh_hi, bb[:, at]) + nn(weigh_lo, bb[:, at])
        out_o[:, at] = (stream[:, at].astype(F32) + part).astype(BF16)

    remote(send.at[pl.ds(0, 63)], recv.at[pl.ds(0, 63)], ssem.at[0], rsem.at[0], facing).wait_send()
    for zs in range(8):
        remote(
            xb.at[pl.ds(32 * zs, 32)], xb.at[pl.ds(256 + 32 * zs, 32)], fsend.at[zs], frecv.at[zs], facing
        ).wait_send()
    for part in range(2):
        span = pl.ds(HALF * part, HALF)
        remote(ypart.at[span], yrecv.at[span], psend.at[part], precv.at[part], facing).wait_send()
    remote(ret.at[pl.ds(0, 63)], bk.at[pl.ds(0, 63)], bsend.at[0], brecv.at[0], facing).wait_send()


def moe(ids, gw, pw, normed, stream, wg, wu, wd, pg, pu, pd):
    vm = pl.BlockSpec(memory_space=pltpu.VMEM)
    hbm = pl.BlockSpec(memory_space=pl.ANY)
    dma = pltpu.SemaphoreType.DMA
    slab = pltpu.VMEM((64, 4, D), BF16)
    return pl.pallas_call(
        moe_kernel,
        name="moe",
        out_shape=jax.ShapeDtypeStruct((96, D), BF16),
        in_specs=[vm] * 5 + [hbm] * 6,
        out_specs=vm,
        scratch_shapes=[
            pltpu.VMEM((2, D, 256), BF16), pltpu.VMEM((2, D, 256), BF16), pltpu.VMEM((2, 256, D), BF16),
            slab, slab, pltpu.VMEM((512, D), BF16), pltpu.VMEM((512, 512), BF16),
            pltpu.VMEM((256, D), F32), pltpu.VMEM((256, D), BF16), pltpu.VMEM((256, D), BF16),
            slab, slab, pltpu.VMEM((256, D), BF16),
            dma((6,)), dma((1,)), dma((8,)), dma((8,)), dma((8,)), dma((2,)), dma((2,)), dma((1,)), dma((1,)),
        ],
        compiler_params=pltpu.CompilerParams(
            collective_id=1, has_side_effects=True, vmem_limit_bytes=48 * 1024 * 1024
        ),
    )(ids, gw, pw, normed, stream, wg, wu, wd, pg, pu, pd)


def body(
    residual, query_one, key_one, value_one, gate_one, decay_one, norm_one, output_one,
    query_two, key_two, value_two, gate_two, decay_two, norm_two, output_two, norm_gain,
    expert_ids, group_weight, pair_weight, expert_gate, expert_up, expert_down,
):
    wg, wu, wd = expert_gate[0], expert_up[0], expert_down[0]
    stream, normed, pg, pu, pd = mixer(
        query_one, key_one, value_one, gate_one, decay_one, norm_one[None],
        query_two, key_two, value_two, gate_two, decay_two, norm_two[None], norm_gain[None],
        residual, output_one, output_two, wg, wu, wd,
    )
    return moe(expert_ids, group_weight[:, None], pair_weight, normed, stream, wg, wu, wd, pg, pu, pd)


def solution(mesh):
    torus = Mesh(mesh.devices.reshape(8, 4, 2, mesh.shape["tp"]), SP_TP)
    heads = P(SP, "tp")
    in_specs = (
        P(SP_TP, None), heads, heads, heads, heads, P(None, SP, "tp"), P(), P("tp", None),
        heads, heads, heads, heads, P(None, SP, "tp"), P(), P("tp", None),
        P(), P(SP, None), P(SP), P(SP, None), P(SP, None, "tp"), P(SP, None, "tp"), P(SP, "tp", None),
    )
    return jax.shard_map(body, mesh=torus, in_specs=in_specs, out_specs=P(SP_TP, None), check_vma=False)
```

```python
import jax
import jax.numpy as jnp
from jax import lax
from jax.experimental import pallas as pl
from jax.experimental.pallas import tpu as pltpu
from jax.sharding import Mesh
from jax.sharding import PartitionSpec as P

D = 2048
BLOCK = 64
NB = 6
KEYS = 384
SP = ("sp_0", "sp_1", "sp_2")
SP_TP = ("sp_0", "sp_1", "sp_2", "tp")
EPS = 1e-06
F32 = jnp.float32
BF16 = jnp.bfloat16


def place():
    return tuple(lax.axis_index(a) for a in SP_TP)


def dev(z, y, c, x):
    return {"sp_0": z, "sp_1": y, "sp_2": c, "tp": x}


def remote(src, dst, ssem, rsem, device):
    return pltpu.make_async_remote_copy(
        src_ref=src,
        dst_ref=dst,
        send_sem=ssem,
        recv_sem=rsem,
        device_id=device,
        device_id_type=pl.DeviceIdType.MESH,
    )


def greet(barrier, device):
    pl.semaphore_signal(barrier, inc=1, device_id=device, device_id_type=pl.DeviceIdType.MESH)


def nn(a, b):
    return lax.dot_general(a, b, (((1,), (0,)), ((), ())), preferred_element_type=F32)


def nt(a, b):
    return lax.dot_general(a, b, (((1,), (1,)), ((), ())), preferred_element_type=F32)


def tn(a, b):
    return lax.dot_general(a, b, (((0,), (0,)), ((), ())), preferred_element_type=F32)


def iota2(shape, dim):
    return lax.broadcasted_iota(jnp.int32, shape, dim)


def halves(row):
    hi = row.astype(BF16)
    lo = (row - hi.astype(F32)).astype(BF16)
    return hi, lo


ORDER = (4, 0, 3, 5, 2, 6, 1, 7)
MIRROR = tuple(ORDER.index((-dz) % 8) for dz in ORDER)
CHUNKS = 4

INPUTS = (
    "res", "q1", "k1", "v1", "g1", "d1", "n1", "ow1", "q2", "k2", "v2", "g2", "d2", "n2", "ow2",
    "ng", "ids", "gw", "pw", "eg", "eu", "ed",
)


def dma(*n):
    return pltpu.SemaphoreType.DMA(n)


def scratch_shapes():
    vm = pltpu.VMEM
    slab = vm((64, 4, D), BF16)
    return {
        "q": vm((384, KEYS), BF16), "k": vm((384, KEYS), BF16), "v": vm((384, 512), BF16),
        "g": vm((384, 512), BF16), "d": vm((2, 384, KEYS), BF16), "gain": vm((1, 256), F32),
        "ngv": vm((1, D), F32), "idv": vm((2, 384), jnp.int32), "gwv": vm((384,), F32),
        "pwv": vm((2, 384), F32), "resv": vm((96, D), BF16), "ow": vm((512, D), BF16),
        "cum": vm((2, 384, KEYS), F32), "qd": vm((2, 384, KEYS), BF16), "kd": vm((2, 384, KEYS), BF16),
        "add": vm((2, NB, 128, KEYS), F32), "dec": vm((2, NB, 8, KEYS), F32),
        "acc": vm((384, 512), F32), "gs": vm((384, 512), F32), "st": vm((2, NB, 128, KEYS), BF16),
        "s1": vm((8, 40, KEYS), BF16), "r1": vm((8, 40, KEYS), BF16),
        "pre": vm((2, 8, 16, KEYS), F32), "prd": vm((2, 8, 8, KEYS), F32),
        "s2": vm((2, 24, KEYS), BF16), "r2": vm((8, 24, KEYS), BF16),
        "s3": vm((8, 32, KEYS), BF16), "r3": vm((8, 32, KEYS), BF16),
        "mixed": vm((384, 512), BF16), "pbuf": vm((4, 96, D), BF16), "prec": vm((4, 96, D), BF16),
        "stream": vm((96, D), BF16), "normed": vm((96, D), BF16),
        "sel": vm((256, 96), BF16), "whi": vm((256, 96), BF16), "wlo": vm((256, 96), BF16),
        "wg": vm((2, D, 256), BF16), "wu": vm((2, D, 256), BF16), "wd": vm((2, 256, D), BF16),
        "send": slab, "recv": slab, "ret": slab, "bk": slab,
        "xb": vm((512, D), BF16), "hid": vm((128, 512), BF16), "yown": vm((256, D), F32),
        "ypart": vm((256, D), BF16), "yrecv": vm((256, D), BF16), "bb": vm((256, D), BF16),
        "lsem": dma(25), "wsend": dma(3), "wrecv": dma(3), "xsem": dma(3), "rsem": dma(3),
        "dsend": dma(4), "drecv": dma(4), "ssem": dma(1), "srecv": dma(CHUNKS),
        "fsend": dma(CHUNKS), "frecv": dma(CHUNKS), "psend": dma(CHUNKS), "precv": dma(CHUNKS),
        "bsend": dma(1), "brecv": dma(CHUNKS),
    }


class Refs:
    def __init__(self, names, refs):
        self.__dict__.update(zip(names, refs))


def layer_kernel(*refs):
    shapes = scratch_shapes()
    r = Refs(INPUTS + ("out",) + tuple(shapes), refs)
    z, y, c, x = place()
    p = y * 2 + c
    sgn = (1 - 2 * (x % 2)) * (1 - 2 * c)
    friend = dev(z, y, c, (x + sgn + 4) % 4)
    facing = dev(z, y, c, (x - sgn + 4) % 4)

    def rank(dz, t):
        return dev((z + dz) % 8, t // 2, t % 2, x)

    plan = {
        "d": [(r.d1, r.d.at[:, :, 0:128]), (r.d2, r.d.at[:, :, 128:384])],
        "k": [(r.k1, r.k.at[:, 0:128]), (r.k2, r.k.at[:, 128:384])],
        "v": [(r.v1, r.v.at[:, 0:256]), (r.v2, r.v.at[:, 256:512])],
        "q": [(r.q1, r.q.at[:, 0:128]), (r.q2, r.q.at[:, 128:384])],
        "g": [(r.g1, r.g.at[:, 0:256]), (r.g2, r.g.at[:, 256:512]),
              (r.n1, r.gain.at[:, 0:128]), (r.n2, r.gain.at[:, 128:256])],
        "i": [(r.ids, r.idv), (r.gw, r.gwv), (r.pw, r.pwv)],
        "o": [(r.ow1, r.ow.at[pl.ds(0, 256)]), (r.ow2, r.ow.at[pl.ds(256, 256)])],
        "s": [(r.res, r.resv), (r.ng, r.ngv)],
        "w": [(r.eg.at[0], r.wg.at[0]), (r.eu.at[0], r.wu.at[0]), (r.ed.at[0], r.wd.at[0])],
    }
    loads, count = {}, 0
    for name, pairs in plan.items():
        loads[name] = []
        for src, dst in pairs:
            cp = pltpu.make_async_copy(src, dst, r.lsem.at[count])
            count += 1
            cp.start()
            loads[name].append(cp)

    def loaded(names):
        for name in names:
            for cp in loads[name]:
                cp.wait()

    barrier = pltpu.get_barrier_semaphore()

    @pl.loop(1, 64)
    def _(o):
        t = (z * 8 + p + o) % 64
        greet(barrier, dev(t // 8, (t // 2) % 4, t % 2, x))

    for o in range(1, 4):
        greet(barrier, dev(z, y, c, (x + o) % 4))

    row = iota2((BLOCK, BLOCK), 0)
    col = iota2((BLOCK, BLOCK), 1)
    lower, upper = row >= col, row <= col
    tri = tuple(jnp.where(m, 1.0, 0.0).astype(BF16) for m in (lower, upper))
    tri = tuple(jnp.concatenate([t, t, t], axis=1) for t in tri)
    scale = jnp.where(iota2((1, KEYS), 1) < 128, 64.0 ** -0.5, 128.0 ** -0.5)
    lane = iota2((1, 256), 1) % 128 < 64
    zero = jnp.zeros((), BF16)
    SPANS = (slice(0, 128), slice(0, 128), slice(128, 256), slice(256, 384))

    def keys_of(n):
        rows = pl.ds(n * BLOCK, BLOCK)
        k = r.k[rows, :].astype(F32)
        ends = []
        for way in range(2):
            d = r.d[way, rows, :].astype(F32)
            rate = (jnp.minimum(d, 0.0) - jnp.log1p(jnp.exp(-jnp.abs(d)))) * (1.0 / 16.0)
            hi = rate.astype(BF16)
            rest = rate - hi.astype(F32)
            mid = rest.astype(BF16)
            low = (rest - mid.astype(F32)).astype(BF16)
            cum = nn(tri[way], jnp.concatenate([hi, mid, low], axis=0))
            r.cum[way, rows, :] = cum
            fade = jnp.exp(cum[BLOCK - 1 :, :] if way == 0 else cum[0:1, :])
            kd = k * jnp.exp(-cum)
            r.kd[way, rows, :] = kd.astype(BF16)
            r.dec[way, n] = jnp.broadcast_to(fade, (8, KEYS))
            ends.append((kd * fade).astype(BF16))
        both = []
        for h, at in enumerate(SPANS):
            v = r.v[rows, 128 * h : 128 * h + 128]
            both.append(tn(v, jnp.concatenate([ends[0][:, at], ends[1][:, at]], axis=1)))
        both[0:2] = [jnp.where(lane, both[0], both[1])]
        for way in range(2):
            for i, b in enumerate(both):
                r.add[way, n, :, 128 * i : 128 * i + 128] = b[:, 128 * way : 128 * way + 128]

    loaded("dkv")
    for n in range(NB):
        keys_of(n)

    pl.semaphore_wait(barrier, 66)
    weights = [
        remote(src.at[0], dst.at[1], r.wsend.at[i], r.wrecv.at[i], friend)
        for i, (src, dst) in enumerate(((r.eg, r.wg), (r.eu, r.wu), (r.ed, r.wd)))
    ]
    weights[0].start()
    weights[1].start()

    totals, fades = [], []
    for way in range(2):
        order = range(NB) if way == 0 else range(NB - 1, -1, -1)
        run, fade = None, None
        for n in order:
            f = r.dec[way, n][0:1]
            run = r.add[way, n] if run is None else run * f + r.add[way, n]
            fade = f if fade is None else fade * f
        totals.append(run.astype(BF16))
        fades.append(fade)
    tile = jnp.concatenate([t.astype(F32) for f in fades for t in halves(f)] * 2, axis=0).astype(BF16)
    for j in range(8):
        r.s1[j, 0:16, :] = totals[0][16 * j : 16 * j + 16]
        r.s1[j, 16:32, :] = totals[1][16 * j : 16 * j + 16]
        r.s1[j, 32:40, :] = tile
    r.r1[p] = r.s1[p]

    def plane_copy(src, dst, i, o):
        t = (p + o) % 8
        return remote(src.at[t], dst.at[p], r.xsem.at[i], r.rsem.at[i], rank(0, t))

    for o in (4, 3, 5, 2, 6, 1, 7):
        plane_copy(r.s1, r.r1, 0, o).start()

    def queries_of(n):
        rows = pl.ds(n * BLOCK, BLOCK)
        q = r.q[rows, :].astype(F32) * scale
        for way in range(2):
            r.qd[way, rows, :] = (q * jnp.exp(r.cum[way, rows, :])).astype(BF16)

    def inner(n):
        rows = pl.ds(n * BLOCK, BLOCK)
        for h, at in enumerate(SPANS):
            m = None if h > 1 else lane[:, 0:128] if h == 0 else jnp.logical_not(lane[:, 0:128])
            s = []
            for way in range(2):
                qd = r.qd[way, rows, at]
                s.append(nt(qd if m is None else jnp.where(m, qd, zero), r.kd[way, rows, at]))
            s = jnp.where(lower, s[0], 0.0) + jnp.where(upper, s[1], 0.0)
            head = slice(128 * h, 128 * h + 128)
            r.acc[rows, head] = nn(s.astype(BF16), r.v[rows, head])

    loaded("q")
    for n in range(NB):
        queries_of(n)
    for n in range(3):
        inner(n)

    def seven(src, dst, i):
        return remote(src.at[pl.ds(0, 7)], dst.at[pl.ds(0, 7)], r.xsem.at[i], r.rsem.at[i], facing)

    batches = [seven(r.s1, r.r1, 0), seven(r.r2, r.r2, 1), seven(r.s3, r.r3, 2)]
    batches[0].wait_recv()

    def unpack(i):
        s = r.r1[i].astype(F32)
        return s[0:16], s[16:32], s[32:33] + s[33:34], s[34:35] + s[35:36]

    parts = [unpack(i) for i in range(8)]
    for way in range(2):
        run, fade = jnp.zeros((16, KEYS), F32), jnp.ones((1, KEYS), F32)
        for i in range(8) if way == 0 else range(7, -1, -1):
            r.pre[way, i] = run
            r.prd[way, i] = jnp.broadcast_to(fade, (8, KEYS))
            run = run * parts[i][2 + way] + parts[i][way]
            fade = fade * parts[i][2 + way]
        hi, lo = halves(fade)
        r.s2[way, 0:16, :] = run.astype(BF16)
        r.s2[way, 16:24, :] = jnp.concatenate([hi.astype(F32), lo.astype(F32)] * 4, axis=0).astype(BF16)
    r.r2[z] = r.s2[0]
    for o in (4, 3, 5, 2, 6, 1, 7):
        remote(r.s2.at[(z + o) // 8], r.r2.at[z], r.xsem.at[1], r.rsem.at[1], rank(o, p)).start()

    for n in range(3, NB):
        inner(n)

    loaded("i")

    def mine(ref):
        pick = ref[:, 288:384]
        for i in (2, 1, 0):
            pick = jnp.where(x == i, ref[:, 96 * i : 96 * i + 96], pick)
        return pick

    ids, gate, pair = mine(r.idv), mine(r.gwv[...][None]), mine(r.pwv)
    inv = gate / (pair[0:1] + pair[1:2])
    experts = iota2((64, 96), 0)
    named = [jnp.where(ids[k : k + 1] == experts, 1.0, 0.0) for k in range(2)]
    before = jnp.where(iota2((96, 96), 0) < iota2((96, 96), 1), 1.0, 0.0).astype(BF16)
    count = nn((named[0] + named[1]).astype(BF16), before)
    slots = [
        jnp.sum(count * named[k], axis=0, keepdims=True).astype(jnp.int32) + 4 * ids[k : k + 1] for k in range(2)
    ]
    for i, dz in enumerate(ORDER):
        here = iota2((32, 96), 0) + 32 * ((z + dz) % 8)
        hits = [jnp.where(slots[k] == here, 1.0, 0.0) for k in range(2)]
        at = slice(32 * i, 32 * i + 32)
        r.sel[at, :] = (hits[0] + hits[1]).astype(BF16)
        r.whi[at, :], r.wlo[at, :] = halves(hits[0] * (inv * pair[0:1]) + hits[1] * (inv * pair[1:2]))

    batches[1].wait_recv()
    entry = []
    for way in range(2):
        run = jnp.zeros((16, KEYS), F32)
        for i in range(8) if way == 0 else range(7, -1, -1):
            s = r.r2[i].astype(F32)
            run = jnp.where(i < z if way == 0 else i > z, run * (s[16:17] + s[17:18]) + s[0:16], run)
        entry.append(run)
    for j in range(8):
        for way in range(2):
            r.s3[j, 16 * way : 16 * way + 16, :] = (
                r.pre[way, j] + r.prd[way, j][0:1] * entry[way]
            ).astype(BF16)
    r.r3[p] = r.s3[p]
    for o in (4, 3, 5, 2, 6, 1, 7):
        plane_copy(r.s3, r.r3, 2, o).start()

    loaded("g")
    for n in range(NB):
        rows = pl.ds(n * BLOCK, BLOCK)
        g = r.g[rows, :].astype(F32)
        gain = r.gain[...]
        gain = jnp.concatenate([gain[:, 0:128], gain[:, 0:128], gain[:, 128:256], gain[:, 128:256]], axis=1)
        r.gs[rows, :] = gain * (g / (1.0 + jnp.exp(-g)))

    batches[2].wait_recv()
    for way in range(2):
        state = jnp.concatenate([r.r3[j, 16 * way : 16 * way + 16, :] for j in range(8)], axis=0).astype(F32)
        for n in range(NB) if way == 0 else range(NB - 1, -1, -1):
            r.st[way, n] = state.astype(BF16)
            state = state * r.dec[way, n][0:1] + r.add[way, n]

    def read_out(n):
        rows = pl.ds(pl.multiple_of(n * BLOCK, BLOCK), BLOCK)
        for h, at in enumerate(SPANS):
            qd = jnp.concatenate([r.qd[0, rows, at], r.qd[1, rows, at]], axis=1)
            if h < 2:
                qd = jnp.where(lane if h == 0 else jnp.logical_not(lane), qd, zero)
            head = slice(128 * h, 128 * h + 128)
            t = r.acc[rows, head] + nt(qd, jnp.concatenate([r.st[0, n, :, at], r.st[1, n, :, at]], axis=1))
            t = t * lax.rsqrt(jnp.mean(t * t, axis=1, keepdims=True) + EPS)
            r.mixed[rows, head] = (t * r.gs[rows, head]).astype(BF16)

    def to_owner(o):
        return remote(r.pbuf.at[o], r.prec.at[o], r.dsend.at[o], r.drecv.at[o], dev(z, y, c, (x + o) % 4))

    def project(t, away):
        o = (t - x + 4) % 4
        rows = r.mixed[pl.ds(pl.multiple_of(t * 96, 32), 96), :]
        for q in range(4):
            at = slice(512 * q, 512 * q + 512)
            r.pbuf[o, :, at] = nn(rows, r.ow[:, at]).astype(BF16)
        if away:
            to_owner(o).start()

    across = (x + 2) % 4
    half = across // 2
    for i in range(3):
        read_out(3 * half + i)
    loaded("o")
    project(across, True)
    project(across + 1 - 2 * (across % 2), True)
    for i in range(3):
        read_out(3 * (1 - half) + i)
    project(x + 1 - 2 * (x % 2), True)
    weights[2].start()
    project(x, False)

    loaded("s")
    for o in (1, 3, 2):
        to_owner(o).wait_recv()
    for q in range(4):
        at = slice(512 * q, 512 * q + 512)
        total = r.pbuf[0, :, at].astype(F32)
        for o in (1, 3, 2):
            total = total + r.prec[o, :, at].astype(F32)
        r.stream[:, at] = (r.resv[:, at].astype(F32) + total.astype(BF16).astype(F32)).astype(BF16)
    wide = r.stream[...].astype(F32)
    ms = jnp.mean(wide * wide, axis=1, keepdims=True)
    r.normed[...] = (wide * lax.rsqrt(ms + EPS) * r.ngv[...]).astype(BF16)

    def scatter_rows(dst, first, rows, at):
        for e in range(rows.shape[0] // 4):
            dst[first + e, :, at] = rows[4 * e : 4 * e + 4, :]

    def slabs_out(src, dst, ssem, rsem, k):
        for i in (2 * k, 2 * k + 1):
            @pl.loop(1 if ORDER[i] == 0 else 0, 8)
            def _(o):
                t = (p + o) % 8
                remote(
                    src.at[i * 8 + t], dst.at[MIRROR[i] * 8 + p], ssem.at[0], rsem.at[k], rank(ORDER[i], t)
                ).start()

    def slabs_in(src, dst, ssem, rsem, k):
        n = 15 if k == 0 else 16
        return remote(src.at[pl.ds(0, n)], dst.at[pl.ds(0, n)], ssem.at[0], rsem.at[k], facing)

    for k in range(CHUNKS):
        for q in range(4):
            at = slice(512 * q, 512 * q + 512)
            rows = nn(r.sel[64 * k : 64 * k + 64, :], r.normed[:, at])
            scatter_rows(r.send, 16 * k, rows.astype(BF16), at)
        if k == 0:
            r.recv[8 + p] = r.send[8 + p]
        slabs_out(r.send, r.recv, r.ssem, r.srecv, k)

    def forward(k):
        return remote(
            r.xb.at[pl.ds(128 * k, 64)], r.xb.at[pl.ds(128 * k + 64, 64)], r.fsend.at[k], r.frecv.at[k], facing
        )

    def partial(k):
        span = pl.ds(64 * k, 64)
        return remote(r.ypart.at[span], r.yrecv.at[span], r.psend.at[k], r.precv.at[k], facing)

    def arrive(k):
        slabs_in(r.send, r.recv, r.ssem, r.srecv, k).wait_recv()
        for i in range(2):
            r.xb[128 * k + 32 * i : 128 * k + 32 * i + 32, :] = jnp.concatenate(
                [r.recv[16 * k + 8 * i + j] for j in range(8)], axis=0
            )
        forward(k).start()

    def experts_on(k):
        if k == 0:
            loaded("w")
            weights[0].wait_recv()
            weights[1].wait_recv()
        forward(k).wait_recv()
        rows = pl.ds(128 * k, 128)
        for s in range(2):
            a = nn(r.xb[rows, :], r.wg[s])
            b = nn(r.xb[rows, :], r.wu[s])
            r.hid[:, 256 * s : 256 * s + 256] = (a / (1.0 + jnp.exp(-a)) * b).astype(BF16)
        if k == 0:
            weights[2].wait_recv()
        for q in range(4):
            at = slice(512 * q, 512 * q + 512)
            out = nn(r.hid[:, 0:256], r.wd[0, :, at]) + nn(r.hid[:, 256:512], r.wd[1, :, at])
            r.yown[64 * k : 64 * k + 64, at] = out[0:64]
            r.ypart[64 * k : 64 * k + 64, at] = out[64:128].astype(BF16)
        partial(k).start()

    def give_back(k):
        partial(k).wait_recv()
        span = slice(64 * k, 64 * k + 64)
        for q in range(4):
            at = slice(512 * q, 512 * q + 512)
            rows = r.yown[span, at] + r.yrecv[span, at].astype(F32)
            scatter_rows(r.ret, 16 * k, rows.astype(BF16), at)
        if k == 0:
            r.bk[8 + p] = r.ret[8 + p]
        slabs_out(r.ret, r.bk, r.bsend, r.brecv, k)

    arrive(0)
    experts_on(0)
    arrive(1)
    experts_on(1)
    give_back(0)
    arrive(2)
    arrive(3)
    give_back(1)
    experts_on(2)
    experts_on(3)
    give_back(2)
    give_back(3)

    def gather_back(k):
        slabs_in(r.ret, r.bk, r.bsend, r.brecv, k).wait_recv()
        for i in range(2):
            r.bb[64 * k + 32 * i : 64 * k + 32 * i + 32, :] = jnp.concatenate(
                [r.bk[16 * k + 8 * i + j] for j in range(8)], axis=0
            )

    def combined(first, last, at):
        return tn(r.whi[first:last, :], r.bb[first:last, at]) + tn(r.wlo[first:last, :], r.bb[first:last, at])

    for k in range(3):
        gather_back(k)
    early = [combined(0, 192, slice(512 * q, 512 * q + 512)) for q in range(4)]
    gather_back(3)
    for q in range(4):
        at = slice(512 * q, 512 * q + 512)
        total = r.stream[:, at].astype(F32) + early[q] + combined(192, 256, at)
        r.out[:, at] = total.astype(BF16)

    for batch in batches:
        batch.wait_send()
    for o in (1, 2, 3):
        to_owner(o).wait_send()
    for cp in weights:
        cp.wait_send()
    for src, dst, ssem, rsem in ((r.send, r.recv, r.ssem, r.srecv), (r.ret, r.bk, r.bsend, r.brecv)):
        remote(src.at[pl.ds(0, 63)], dst.at[pl.ds(0, 63)], ssem.at[0], rsem.at[0], facing).wait_send()
    for k in range(CHUNKS):
        forward(k).wait_send()
        partial(k).wait_send()


def body(
    residual, query_one, key_one, value_one, gate_one, decay_one, norm_one, output_one,
    query_two, key_two, value_two, gate_two, decay_two, norm_two, output_two, norm_gain,
    expert_ids, group_weight, pair_weight, expert_gate, expert_up, expert_down,
):
    return pl.pallas_call(
        layer_kernel,
        name="layer",
        out_shape=jax.ShapeDtypeStruct((96, D), BF16),
        in_specs=[pl.BlockSpec(memory_space=pltpu.HBM)] * len(INPUTS),
        out_specs=pl.BlockSpec(memory_space=pltpu.VMEM),
        scratch_shapes=list(scratch_shapes().values()),
        compiler_params=pltpu.CompilerParams(
            collective_id=0, has_side_effects=True, vmem_limit_bytes=60 * 1024 * 1024
        ),
    )(
        residual, query_one, key_one, value_one, gate_one, decay_one, norm_one[None], output_one,
        query_two, key_two, value_two, gate_two, decay_two, norm_two[None], output_two, norm_gain[None],
        expert_ids.T, group_weight, pair_weight.T, expert_gate, expert_up, expert_down,
    )


def solution(mesh):
    torus = Mesh(mesh.devices.reshape(8, 4, 2, mesh.shape["tp"]), SP_TP)
    heads = P(SP, "tp")
    in_specs = (
        P(SP_TP, None), heads, heads, heads, heads, P(None, SP, "tp"), P(), P("tp", None),
        heads, heads, heads, heads, P(None, SP, "tp"), P(), P("tp", None),
        P(), P(SP, None), P(SP), P(SP, None), P(SP, None, "tp"), P(SP, None, "tp"), P(SP, "tp", None),
    )
    return jax.shard_map(body, mesh=torus, in_specs=in_specs, out_specs=P(SP_TP, None), check_vma=False)
```

```python
import jax
import jax.numpy as jnp
from jax import lax
from jax.experimental import pallas as pl
from jax.experimental.pallas import tpu as pltpu
from jax.sharding import Mesh
from jax.sharding import PartitionSpec as P

D = 2048
BLOCK = 64
NB = 6
KEYS = 384
SP = ("sp_0", "sp_1", "sp_2")
SP_TP = ("sp_0", "sp_1", "sp_2", "tp")
EPS = 1e-06
F32 = jnp.float32
BF16 = jnp.bfloat16


def place():
    return tuple(lax.axis_index(a) for a in SP_TP)


def dev(z, y, c, x):
    return {"sp_0": z, "sp_1": y, "sp_2": c, "tp": x}


def remote(src, dst, ssem, rsem, device):
    return pltpu.make_async_remote_copy(
        src_ref=src,
        dst_ref=dst,
        send_sem=ssem,
        recv_sem=rsem,
        device_id=device,
        device_id_type=pl.DeviceIdType.MESH,
    )


def greet(barrier, device):
    pl.semaphore_signal(barrier, inc=1, device_id=device, device_id_type=pl.DeviceIdType.MESH)


def nn(a, b):
    return lax.dot_general(a, b, (((1,), (0,)), ((), ())), preferred_element_type=F32)


def nt(a, b):
    return lax.dot_general(a, b, (((1,), (1,)), ((), ())), preferred_element_type=F32)


def tn(a, b):
    return lax.dot_general(a, b, (((0,), (0,)), ((), ())), preferred_element_type=F32)


def iota2(shape, dim):
    return lax.broadcasted_iota(jnp.int32, shape, dim)


def halves(row):
    hi = row.astype(BF16)
    lo = (row - hi.astype(F32)).astype(BF16)
    return hi, lo


ORDER = (4, 0, 3, 5, 2, 6, 1, 7)
MIRROR = tuple(ORDER.index((-dz) % 8) for dz in ORDER)
CHUNKS = 4
HALF = D // 2

INPUTS = (
    "res", "q1", "k1", "v1", "g1", "d1", "n1", "ow1", "q2", "k2", "v2", "g2", "d2", "n2", "ow2",
    "ng", "ids", "gw", "pw", "eg", "eu", "ed",
)


def dma(*n):
    return pltpu.SemaphoreType.DMA(n)


def scratch_shapes():
    vm = pltpu.VMEM
    slab = vm((64, 4, D), BF16)
    return {
        "q": vm((384, KEYS), BF16), "k": vm((384, KEYS), BF16), "v": vm((384, 512), BF16),
        "g": vm((384, 512), BF16), "d": vm((2, 384, KEYS), BF16), "gain": vm((1, 256), F32),
        "ngv": vm((1, D), F32), "idv": vm((2, 384), jnp.int32), "gwv": vm((384,), F32),
        "pwv": vm((2, 384), F32), "resv": vm((96, D), BF16), "ow": vm((512, D), BF16),
        "cum": vm((2, 384, KEYS), F32), "qd": vm((2, 384, KEYS), BF16), "kd": vm((2, 384, KEYS), BF16),
        "add": vm((2, NB, 128, KEYS), F32), "dec": vm((2, NB, 8, KEYS), F32),
        "acc": vm((384, 512), F32), "gs": vm((384, 512), F32), "st": vm((2, NB, 128, KEYS), BF16),
        "s1": vm((8, 40, KEYS), BF16), "r1": vm((8, 40, KEYS), BF16),
        "pre": vm((2, 8, 16, KEYS), F32), "prd": vm((2, 8, 8, KEYS), F32),
        "s2": vm((2, 24, KEYS), BF16), "r2": vm((8, 24, KEYS), BF16),
        "s3": vm((8, 32, KEYS), BF16), "r3": vm((8, 32, KEYS), BF16),
        "mixed": vm((384, 512), BF16), "pbuf": vm((2, 4, 96, HALF), BF16), "prec": vm((2, 2, 96, HALF), BF16), "hop": vm((2, 2, 48, HALF), BF16),
        "stream": vm((96, D), BF16), "oacc": vm((96, D), F32),
        "sel": vm((256, 96), BF16), "whi": vm((256, 96), BF16), "wlo": vm((256, 96), BF16),
        "wg": vm((2, D, 256), BF16), "wu": vm((2, D, 256), BF16), "wd": vm((2, 256, D), BF16),
        "send0": vm((64, 4, HALF), BF16), "recv0": vm((64, 4, HALF), BF16),
        "send1": vm((64, 4, HALF + 128), BF16), "recv1": vm((64, 4, HALF + 128), BF16), "ret": slab, "bk": slab,
        "xb": vm((512, D), BF16), "hid": vm((128, 512), BF16), "yown": vm((256, D), F32),
        "ypart": vm((256, D), BF16), "yrecv": vm((256, D), BF16), "bb": vm((256, D), BF16),
        "lsem": dma(25), "wsend": dma(4), "wrecv": dma(4), "xsem": dma(3), "rsem": dma(3),
        "dsend": dma(8), "drecv": dma(8), "hsend": dma(4), "hrecv": dma(4), "ssem": dma(2), "srecv": dma(2 * CHUNKS),
        "fsend": dma(CHUNKS), "frecv": dma(CHUNKS), "psend": dma(CHUNKS), "precv": dma(CHUNKS),
        "bsend": dma(1), "brecv": dma(CHUNKS),
    }


class Refs:
    def __init__(self, names, refs):
        self.__dict__.update(zip(names, refs))


def layer_kernel(*refs):
    shapes = scratch_shapes()
    r = Refs(INPUTS + ("out",) + tuple(shapes), refs)
    z, y, c, x = place()
    p = y * 2 + c
    sgn = (1 - 2 * (x % 2)) * (1 - 2 * c)
    friend = dev(z, y, c, (x + sgn + 4) % 4)
    facing = dev(z, y, c, (x - sgn + 4) % 4)

    def rank(dz, t):
        return dev((z + dz) % 8, t // 2, t % 2, x)

    plan = {
        "d": [(r.d1, r.d.at[:, :, 0:128]), (r.d2, r.d.at[:, :, 128:384])],
        "k": [(r.k1, r.k.at[:, 0:128]), (r.k2, r.k.at[:, 128:384])],
        "v": [(r.v1, r.v.at[:, 0:256]), (r.v2, r.v.at[:, 256:512])],
        "q": [(r.q1, r.q.at[:, 0:128]), (r.q2, r.q.at[:, 128:384])],
        "g": [(r.g1, r.g.at[:, 0:256]), (r.g2, r.g.at[:, 256:512]),
              (r.n1, r.gain.at[:, 0:128]), (r.n2, r.gain.at[:, 128:256])],
        "i": [(r.ids, r.idv), (r.gw, r.gwv), (r.pw, r.pwv)],
        "o": [(r.ow1, r.ow.at[pl.ds(0, 256)]), (r.ow2, r.ow.at[pl.ds(256, 256)])],
        "s": [(r.res, r.resv), (r.ng, r.ngv)],
        "w": [(r.eg.at[0], r.wg.at[0]), (r.eu.at[0], r.wu.at[0]), (r.ed.at[0], r.wd.at[0])],
    }
    loads, count = {}, 0
    for name, pairs in plan.items():
        loads[name] = []
        for src, dst in pairs:
            cp = pltpu.make_async_copy(src, dst, r.lsem.at[count])
            count += 1
            cp.start()
            loads[name].append(cp)

    def loaded(names):
        for name in names:
            for cp in loads[name]:
                cp.wait()

    barrier = pltpu.get_barrier_semaphore()

    @pl.loop(1, 64)
    def _(o):
        t = (z * 8 + p + o) % 64
        greet(barrier, dev(t // 8, (t // 2) % 4, t % 2, x))

    for o in range(1, 4):
        greet(barrier, dev(z, y, c, (x + o) % 4))

    row = iota2((BLOCK, BLOCK), 0)
    col = iota2((BLOCK, BLOCK), 1)
    lower, upper = row >= col, row <= col
    tri = tuple(jnp.where(m, 1.0, 0.0).astype(BF16) for m in (lower, upper))
    tri = tuple(jnp.concatenate([t, t, t], axis=1) for t in tri)
    scale = jnp.where(iota2((1, KEYS), 1) < 128, 64.0 ** -0.5, 128.0 ** -0.5)
    lane = iota2((1, 256), 1) % 128 < 64
    zero = jnp.zeros((), BF16)
    SPANS = (slice(0, 128), slice(0, 128), slice(128, 256), slice(256, 384))

    def keys_of(n):
        rows = pl.ds(n * BLOCK, BLOCK)
        k = r.k[rows, :].astype(F32)
        ends = []
        for way in range(2):
            d = r.d[way, rows, :].astype(F32)
            rate = (jnp.minimum(d, 0.0) - jnp.log1p(jnp.exp(-jnp.abs(d)))) * (1.0 / 16.0)
            hi = rate.astype(BF16)
            rest = rate - hi.astype(F32)
            mid = rest.astype(BF16)
            low = (rest - mid.astype(F32)).astype(BF16)
            cum = nn(tri[way], jnp.concatenate([hi, mid, low], axis=0))
            r.cum[way, rows, :] = cum
            fade = jnp.exp(cum[BLOCK - 1 :, :] if way == 0 else cum[0:1, :])
            kd = k * jnp.exp(-cum)
            r.kd[way, rows, :] = kd.astype(BF16)
            r.dec[way, n] = jnp.broadcast_to(fade, (8, KEYS))
            ends.append((kd * fade).astype(BF16))
        both = []
        for h, at in enumerate(SPANS):
            v = r.v[rows, 128 * h : 128 * h + 128]
            both.append(tn(v, jnp.concatenate([ends[0][:, at], ends[1][:, at]], axis=1)))
        both[0:2] = [jnp.where(lane, both[0], both[1])]
        for way in range(2):
            for i, b in enumerate(both):
                r.add[way, n, :, 128 * i : 128 * i + 128] = b[:, 128 * way : 128 * way + 128]

    loaded("dkv")
    for n in range(NB):
        keys_of(n)

    pl.semaphore_wait(barrier, 66)
    weights = [
        remote(src, dst, r.wsend.at[i], r.wrecv.at[i], friend)
        for i, (src, dst) in enumerate((
            (r.eg.at[0], r.wg.at[1]),
            (r.eu.at[0, pl.ds(0, HALF)], r.wu.at[1, pl.ds(0, HALF)]),
            (r.eu.at[0, pl.ds(HALF, HALF)], r.wu.at[1, pl.ds(HALF, HALF)]),
            (r.ed.at[0], r.wd.at[1]),
        ))
    ]
    weights[0].start()
    weights[1].start()

    totals, fades = [], []
    for way in range(2):
        order = range(NB) if way == 0 else range(NB - 1, -1, -1)
        run, fade = None, None
        for n in order:
            f = r.dec[way, n][0:1]
            run = r.add[way, n] if run is None else run * f + r.add[way, n]
            fade = f if fade is None else fade * f
        totals.append(run.astype(BF16))
        fades.append(fade)
    tile = jnp.concatenate([t.astype(F32) for f in fades for t in halves(f)] * 2, axis=0).astype(BF16)
    for j in range(8):
        r.s1[j, 0:16, :] = totals[0][16 * j : 16 * j + 16]
        r.s1[j, 16:32, :] = totals[1][16 * j : 16 * j + 16]
        r.s1[j, 32:40, :] = tile
    r.r1[p] = r.s1[p]

    def plane_copy(src, dst, i, o):
        t = (p + o) % 8
        return remote(src.at[t], dst.at[p], r.xsem.at[i], r.rsem.at[i], rank(0, t))

    for o in (4, 3, 5, 2, 6, 1, 7):
        plane_copy(r.s1, r.r1, 0, o).start()

    def queries_of(n):
        rows = pl.ds(n * BLOCK, BLOCK)
        q = r.q[rows, :].astype(F32) * scale
        for way in range(2):
            r.qd[way, rows, :] = (q * jnp.exp(r.cum[way, rows, :])).astype(BF16)

    def inner(n):
        rows = pl.ds(n * BLOCK, BLOCK)
        for h, at in enumerate(SPANS):
            m = None if h > 1 else lane[:, 0:128] if h == 0 else jnp.logical_not(lane[:, 0:128])
            s = []
            for way in range(2):
                qd = r.qd[way, rows, at]
                s.append(nt(qd if m is None else jnp.where(m, qd, zero), r.kd[way, rows, at]))
            s = jnp.where(lower, s[0], 0.0) + jnp.where(upper, s[1], 0.0)
            head = slice(128 * h, 128 * h + 128)
            r.acc[rows, head] = nn(s.astype(BF16), r.v[rows, head])

    loaded("q")
    for n in range(NB):
        queries_of(n)
    for n in range(3):
        inner(n)

    def seven(src, dst, i):
        return remote(src.at[pl.ds(0, 7)], dst.at[pl.ds(0, 7)], r.xsem.at[i], r.rsem.at[i], facing)

    batches = [seven(r.s1, r.r1, 0), seven(r.r2, r.r2, 1), seven(r.s3, r.r3, 2)]
    batches[0].wait_recv()

    def unpack(i):
        s = r.r1[i].astype(F32)
        return s[0:16], s[16:32], s[32:33] + s[33:34], s[34:35] + s[35:36]

    parts = [unpack(i) for i in range(8)]
    for way in range(2):
        run, fade = jnp.zeros((16, KEYS), F32), jnp.ones((1, KEYS), F32)
        for i in range(8) if way == 0 else range(7, -1, -1):
            r.pre[way, i] = run
            r.prd[way, i] = jnp.broadcast_to(fade, (8, KEYS))
            run = run * parts[i][2 + way] + parts[i][way]
            fade = fade * parts[i][2 + way]
        hi, lo = halves(fade)
        r.s2[way, 0:16, :] = run.astype(BF16)
        r.s2[way, 16:24, :] = jnp.concatenate([hi.astype(F32), lo.astype(F32)] * 4, axis=0).astype(BF16)
    r.r2[z] = r.s2[0]
    for o in (4, 3, 5, 2, 6, 1, 7):
        remote(r.s2.at[(z + o) // 8], r.r2.at[z], r.xsem.at[1], r.rsem.at[1], rank(o, p)).start()

    for n in range(3, NB):
        inner(n)

    loaded("i")

    def mine(ref):
        pick = ref[:, 288:384]
        for i in (2, 1, 0):
            pick = jnp.where(x == i, ref[:, 96 * i : 96 * i + 96], pick)
        return pick

    ids, gate, pair = mine(r.idv), mine(r.gwv[...][None]), mine(r.pwv)
    inv = gate / (pair[0:1] + pair[1:2])
    experts = iota2((64, 96), 0)
    named = [jnp.where(ids[k : k + 1] == experts, 1.0, 0.0) for k in range(2)]
    before = jnp.where(iota2((96, 96), 0) < iota2((96, 96), 1), 1.0, 0.0).astype(BF16)
    count = nn((named[0] + named[1]).astype(BF16), before)
    slots = [
        jnp.sum(count * named[k], axis=0, keepdims=True).astype(jnp.int32) + 4 * ids[k : k + 1] for k in range(2)
    ]
    for i, dz in enumerate(ORDER):
        here = iota2((32, 96), 0) + 32 * ((z + dz) % 8)
        hits = [jnp.where(slots[k] == here, 1.0, 0.0) for k in range(2)]
        at = slice(32 * i, 32 * i + 32)
        r.sel[at, :] = (hits[0] + hits[1]).astype(BF16)
        r.whi[at, :], r.wlo[at, :] = halves(hits[0] * (inv * pair[0:1]) + hits[1] * (inv * pair[1:2]))

    batches[1].wait_recv()
    entry = []
    for way in range(2):
        run = jnp.zeros((16, KEYS), F32)
        for i in range(8) if way == 0 else range(7, -1, -1):
            s = r.r2[i].astype(F32)
            run = jnp.where(i < z if way == 0 else i > z, run * (s[16:17] + s[17:18]) + s[0:16], run)
        entry.append(run)
    for j in range(8):
        for way in range(2):
            r.s3[j, 16 * way : 16 * way + 16, :] = (
                r.pre[way, j] + r.prd[way, j][0:1] * entry[way]
            ).astype(BF16)
    r.r3[p] = r.s3[p]
    for o in (4, 3, 5, 2, 6, 1, 7):
        plane_copy(r.s3, r.r3, 2, o).start()

    loaded("g")
    for n in range(NB):
        rows = pl.ds(n * BLOCK, BLOCK)
        g = r.g[rows, :].astype(F32)
        gain = r.gain[...]
        gain = jnp.concatenate([gain[:, 0:128], gain[:, 0:128], gain[:, 128:256], gain[:, 128:256]], axis=1)
        r.gs[rows, :] = gain * (g / (1.0 + jnp.exp(-g)))

    batches[2].wait_recv()
    for way in range(2):
        state = jnp.concatenate([r.r3[j, 16 * way : 16 * way + 16, :] for j in range(8)], axis=0).astype(F32)
        for n in range(NB) if way == 0 else range(NB - 1, -1, -1):
            r.st[way, n] = state.astype(BF16)
            state = state * r.dec[way, n][0:1] + r.add[way, n]

    def read_out(n):
        rows = pl.ds(pl.multiple_of(n * BLOCK, BLOCK), BLOCK)
        for h, at in enumerate(SPANS):
            qd = jnp.concatenate([r.qd[0, rows, at], r.qd[1, rows, at]], axis=1)
            if h < 2:
                qd = jnp.where(lane if h == 0 else jnp.logical_not(lane), qd, zero)
            head = slice(128 * h, 128 * h + 128)
            t = r.acc[rows, head] + nt(qd, jnp.concatenate([r.st[0, n, :, at], r.st[1, n, :, at]], axis=1))
            t = t * lax.rsqrt(jnp.mean(t * t, axis=1, keepdims=True) + EPS)
            r.mixed[rows, head] = (t * r.gs[rows, head]).astype(BF16)

    def beside(side):
        return dev(z, y, c, (x + 1 + 2 * side) % 4)

    def band(i):
        return pl.ds(pl.multiple_of(48 * i, 16), 48)

    def hop_copy(cs, side):
        i = 2 * cs + side
        return remote(r.pbuf.at[cs, 3, band(side)], r.hop.at[cs, side], r.hsend.at[i], r.hrecv.at[i], beside(side))

    def owner_copy(cs, side, merged):
        rows = band(side if merged else 1 - side)
        i = 4 * cs + 2 * side + (1 if merged else 0)
        return remote(r.pbuf.at[cs, 1 + side, rows], r.prec.at[cs, side, rows], r.dsend.at[i], r.drecv.at[i], beside(side))

    def project(t, slot, cs):
        rows = r.mixed[pl.ds(pl.multiple_of(t * 96, 32), 96), :]
        for q in range(2):
            at = slice(512 * q, 512 * q + 512)
            r.pbuf[cs, slot, :, at] = nn(rows, r.ow[:, HALF * cs + 512 * q : HALF * cs + 512 * q + 512]).astype(BF16)

    def to_neighbour(side, cs):
        project((x + 1 + 2 * side) % 4, 1 + side, cs)
        owner_copy(cs, side, False).start()

    def merge(cs, side):
        hop_copy(cs, side).wait_recv()
        rows = band(side)
        for q in range(2):
            at = slice(512 * q, 512 * q + 512)
            both = r.pbuf[cs, 1 + side, rows, at].astype(F32) + r.hop[cs, side, :, at].astype(F32)
            r.pbuf[cs, 1 + side, rows, at] = both.astype(BF16)
        owner_copy(cs, side, True).start()

    def own_rows(cs):
        for side in range(2):
            for merged in (False, True):
                owner_copy(cs, side, merged).wait_recv()
        for q in range(2):
            at = slice(512 * q, 512 * q + 512)
            wide = slice(HALF * cs + 512 * q, HALF * cs + 512 * q + 512)
            total = r.pbuf[cs, 0, :, at].astype(F32)
            for side in range(2):
                total = total + r.prec[cs, side, :, at].astype(F32)
            r.stream[:, wide] = (r.resv[:, wide].astype(F32) + total.astype(BF16).astype(F32)).astype(BF16)

    across = (x + 2) % 4
    half = across // 2
    near = 1 - x % 2
    far = 1 - near
    for i in range(3):
        read_out(3 * half + i)
    loaded("o")
    project(across, 3, 0)
    hop_copy(0, 0).start()
    hop_copy(0, 1).start()
    for i in range(3):
        read_out(3 * (1 - half) + i)
    to_neighbour(near, 0)
    to_neighbour(far, 0)
    project(across, 3, 1)
    hop_copy(1, 0).start()
    hop_copy(1, 1).start()
    merge(0, near)
    merge(0, far)
    to_neighbour(near, 1)
    to_neighbour(far, 1)
    project(x, 0, 0)
    project(x, 0, 1)
    merge(1, near)
    merge(1, far)
    weights[2].start()
    weights[3].start()
    loaded("s")

    def scatter_rows(dst, first, rows, at):
        for e in range(rows.shape[0] // 4):
            dst[first + e, :, at] = rows[4 * e : 4 * e + 4, :]

    def slabs_out(src, dst, ssem, rsem, k):
        for i in (2 * k, 2 * k + 1):
            @pl.loop(1 if ORDER[i] == 0 else 0, 8)
            def _(o):
                t = (p + o) % 8
                remote(src.at[i * 8 + t], dst.at[MIRROR[i] * 8 + p], ssem, rsem, rank(ORDER[i], t)).start()

    def slabs_in(src, dst, ssem, rsem, k):
        n = 15 if k == 0 else 16
        return remote(src.at[pl.ds(0, n)], dst.at[pl.ds(0, n)], ssem, rsem, facing)

    sides = ((r.send0, r.recv0), (r.send1, r.recv1))

    def fill(cs, k):
        span = slice(64 * k, 64 * k + 64)
        for q in range(2):
            at = slice(512 * q, 512 * q + 512)
            rows = nn(r.sel[span, :], r.stream[:, HALF * cs + 512 * q : HALF * cs + 512 * q + 512])
            scatter_rows(sides[cs][0], 16 * k, rows.astype(BF16), at)
        if cs:
            scatter_rows(r.send1, 16 * k, nn(r.sel[span, :], scales).astype(BF16), slice(HALF, HALF + 128))
        if k == 0:
            sides[cs][1][8 + p] = sides[cs][0][8 + p]

    def dispatch(cs, k):
        slabs_out(*sides[cs], r.ssem.at[cs], r.srecv.at[4 * cs + k], k)

    own_rows(0)
    fill(0, 0)
    dispatch(0, 0)
    fill(0, 1)
    dispatch(0, 1)
    fill(0, 2)
    fill(0, 3)
    own_rows(1)
    wide = r.stream[...].astype(F32)
    inv_rms = lax.rsqrt(jnp.mean(wide * wide, axis=1, keepdims=True) + EPS)
    hi = inv_rms.astype(BF16).astype(F32)
    mid = (inv_rms - hi).astype(BF16).astype(F32)
    low = inv_rms - hi - mid
    which = iota2((96, 128), 1)
    scales = jnp.where(which == 0, hi, jnp.where(which == 1, mid, jnp.where(which == 2, low, 0.0))).astype(BF16)
    fill(1, 0)
    dispatch(1, 0)
    fill(1, 1)
    dispatch(1, 1)
    dispatch(0, 2)
    dispatch(0, 3)
    fill(1, 2)
    dispatch(1, 2)
    fill(1, 3)
    dispatch(1, 3)
    r.oacc[...] = wide

    def forward(k):
        return remote(
            r.xb.at[pl.ds(128 * k, 64)], r.xb.at[pl.ds(128 * k + 64, 64)], r.fsend.at[k], r.frecv.at[k], facing
        )

    def partial(k):
        span = pl.ds(64 * k, 64)
        return remote(r.ypart.at[span], r.yrecv.at[span], r.psend.at[k], r.precv.at[k], facing)

    def arrive(k):
        for cs in range(2):
            slabs_in(*sides[cs], r.ssem.at[cs], r.srecv.at[4 * cs + k], k).wait_recv()
        for i in range(2):
            rows = slice(128 * k + 32 * i, 128 * k + 32 * i + 32)
            first, last = (
                jnp.concatenate([ref[16 * k + 8 * i + j] for j in range(8)], axis=0).astype(F32)
                for ref in (r.recv0, r.recv1)
            )
            inv_rms = jnp.sum(last[:, HALF:], axis=1, keepdims=True)
            r.xb[rows, 0:HALF] = (first * inv_rms * r.ngv[:, 0:HALF]).astype(BF16)
            r.xb[rows, HALF:D] = (last[:, 0:HALF] * inv_rms * r.ngv[:, HALF:D]).astype(BF16)
        forward(k).start()

    def experts_on(k):
        if k == 0:
            loaded("w")
            for cp in weights[0:3]:
                cp.wait_recv()
        forward(k).wait_recv()
        rows = pl.ds(128 * k, 128)
        for s in range(2):
            a = nn(r.xb[rows, :], r.wg[s])
            b = nn(r.xb[rows, :], r.wu[s])
            r.hid[:, 256 * s : 256 * s + 256] = (a / (1.0 + jnp.exp(-a)) * b).astype(BF16)
        if k == 0:
            weights[3].wait_recv()
        for q in range(4):
            at = slice(512 * q, 512 * q + 512)
            out = nn(r.hid[:, 0:256], r.wd[0, :, at]) + nn(r.hid[:, 256:512], r.wd[1, :, at])
            r.yown[64 * k : 64 * k + 64, at] = out[0:64]
            r.ypart[64 * k : 64 * k + 64, at] = out[64:128].astype(BF16)
        partial(k).start()

    def give_back(k):
        partial(k).wait_recv()
        span = slice(64 * k, 64 * k + 64)
        for q in range(4):
            at = slice(512 * q, 512 * q + 512)
            rows = r.yown[span, at] + r.yrecv[span, at].astype(F32)
            scatter_rows(r.ret, 16 * k, rows.astype(BF16), at)
        if k == 0:
            r.bk[8 + p] = r.ret[8 + p]
        slabs_out(r.ret, r.bk, r.bsend.at[0], r.brecv.at[k], k)

    arrive(0)
    arrive(1)
    experts_on(0)
    experts_on(1)
    give_back(0)
    arrive(2)
    arrive(3)
    give_back(1)
    experts_on(2)
    experts_on(3)
    give_back(2)
    give_back(3)

    def gather_back(k):
        slabs_in(r.ret, r.bk, r.bsend.at[0], r.brecv.at[k], k).wait_recv()
        for i in range(2):
            r.bb[64 * k + 32 * i : 64 * k + 32 * i + 32, :] = jnp.concatenate(
                [r.bk[16 * k + 8 * i + j] for j in range(8)], axis=0
            )

    for k in range(CHUNKS):
        gather_back(k)
        span = slice(64 * k, 64 * k + 64)
        for q in range(4):
            at = slice(512 * q, 512 * q + 512)
            total = r.oacc[:, at] + tn(r.whi[span, :], r.bb[span, at]) + tn(r.wlo[span, :], r.bb[span, at])
            if k < CHUNKS - 1:
                r.oacc[:, at] = total
            else:
                r.out[:, at] = total.astype(BF16)

    for batch in batches:
        batch.wait_send()
    for cs in range(2):
        for side in range(2):
            hop_copy(cs, side).wait_send()
            for merged in (False, True):
                owner_copy(cs, side, merged).wait_send()
    for cp in weights:
        cp.wait_send()
    for src, dst, ssem, rsem in (
        (r.send0, r.recv0, r.ssem.at[0], r.srecv.at[0]),
        (r.send1, r.recv1, r.ssem.at[1], r.srecv.at[4]),
        (r.ret, r.bk, r.bsend.at[0], r.brecv.at[0]),
    ):
        remote(src.at[pl.ds(0, 63)], dst.at[pl.ds(0, 63)], ssem, rsem, facing).wait_send()
    for k in range(CHUNKS):
        forward(k).wait_send()
        partial(k).wait_send()


def body(
    residual, query_one, key_one, value_one, gate_one, decay_one, norm_one, output_one,
    query_two, key_two, value_two, gate_two, decay_two, norm_two, output_two, norm_gain,
    expert_ids, group_weight, pair_weight, expert_gate, expert_up, expert_down,
):
    return pl.pallas_call(
        layer_kernel,
        name="layer",
        out_shape=jax.ShapeDtypeStruct((96, D), BF16),
        in_specs=[pl.BlockSpec(memory_space=pltpu.HBM)] * len(INPUTS),
        out_specs=pl.BlockSpec(memory_space=pltpu.VMEM),
        scratch_shapes=list(scratch_shapes().values()),
        compiler_params=pltpu.CompilerParams(
            collective_id=0, has_side_effects=True, vmem_limit_bytes=60 * 1024 * 1024
        ),
    )(
        residual, query_one, key_one, value_one, gate_one, decay_one, norm_one[None], output_one,
        query_two, key_two, value_two, gate_two, decay_two, norm_two[None], output_two, norm_gain[None],
        expert_ids.T, group_weight, pair_weight.T, expert_gate, expert_up, expert_down,
    )


def solution(mesh):
    torus = Mesh(mesh.devices.reshape(8, 4, 2, mesh.shape["tp"]), SP_TP)
    heads = P(SP, "tp")
    in_specs = (
        P(SP_TP, None), heads, heads, heads, heads, P(None, SP, "tp"), P(), P("tp", None),
        heads, heads, heads, heads, P(None, SP, "tp"), P(), P("tp", None),
        P(), P(SP, None), P(SP), P(SP, None), P(SP, None, "tp"), P(SP, None, "tp"), P(SP, "tp", None),
    )
    return jax.shard_map(body, mesh=torus, in_specs=in_specs, out_specs=P(SP_TP, None), check_vma=False)
```

```python
import jax
import jax.numpy as jnp
from jax import lax
from jax.experimental import pallas as pl
from jax.experimental.pallas import tpu as pltpu
from jax.sharding import Mesh
from jax.sharding import PartitionSpec as P

D = 2048
BLOCK = 64
NB = 6
KEYS = 384
SP = ("sp_0", "sp_1", "sp_2")
SP_TP = ("sp_0", "sp_1", "sp_2", "tp")
EPS = 1e-06
F32 = jnp.float32
BF16 = jnp.bfloat16


def place():
    return tuple(lax.axis_index(a) for a in SP_TP)


def dev(z, y, c, x):
    return {"sp_0": z, "sp_1": y, "sp_2": c, "tp": x}


def remote(src, dst, ssem, rsem, device):
    return pltpu.make_async_remote_copy(
        src_ref=src,
        dst_ref=dst,
        send_sem=ssem,
        recv_sem=rsem,
        device_id=device,
        device_id_type=pl.DeviceIdType.MESH,
    )


def greet(barrier, device):
    pl.semaphore_signal(barrier, inc=1, device_id=device, device_id_type=pl.DeviceIdType.MESH)


def nn(a, b):
    return lax.dot_general(a, b, (((1,), (0,)), ((), ())), preferred_element_type=F32)


def nt(a, b):
    return lax.dot_general(a, b, (((1,), (1,)), ((), ())), preferred_element_type=F32)


def tn(a, b):
    return lax.dot_general(a, b, (((0,), (0,)), ((), ())), preferred_element_type=F32)


def iota2(shape, dim):
    return lax.broadcasted_iota(jnp.int32, shape, dim)


def halves(row):
    hi = row.astype(BF16)
    lo = (row - hi.astype(F32)).astype(BF16)
    return hi, lo


ORDER = (4, 0, 3, 5, 2, 6, 1, 7)
MIRROR = tuple(ORDER.index((-dz) % 8) for dz in ORDER)
CHUNKS = 4
HALF = D // 2

INPUTS = (
    "res", "q1", "k1", "v1", "g1", "d1", "n1", "ow1", "q2", "k2", "v2", "g2", "d2", "n2", "ow2",
    "ng", "ids", "gw", "pw", "eg", "eu", "ed",
)


def dma(*n):
    return pltpu.SemaphoreType.DMA(n)


def scratch_shapes():
    vm = pltpu.VMEM
    slab = vm((64, 4, D), BF16)
    return {
        "q": vm((384, KEYS), BF16), "k": vm((384, KEYS), BF16), "v": vm((384, 512), BF16),
        "g": vm((384, 512), BF16), "d": vm((2, 384, KEYS), BF16), "gain": vm((1, 256), F32),
        "ngv": vm((1, D), F32), "idv": vm((2, 384), jnp.int32), "gwv": vm((384,), F32),
        "pwv": vm((2, 384), F32), "resv": vm((96, D), BF16), "ow": vm((512, D), BF16),
        "cum": vm((2, 384, KEYS), F32), "qd": vm((2, 384, KEYS), BF16), "kd": vm((2, 384, KEYS), BF16),
        "add": vm((2, NB, 128, KEYS), F32), "dec": vm((2, NB, 8, KEYS), F32),
        "acc": vm((384, 512), F32), "gs": vm((384, 512), F32), "st": vm((2, NB, 128, KEYS), BF16),
        "s1": vm((8, 40, KEYS), BF16), "r1": vm((8, 40, KEYS), BF16),
        "pre": vm((2, 8, 16, KEYS), F32), "prd": vm((2, 8, 8, KEYS), F32),
        "s2": vm((2, 24, KEYS), BF16), "r2": vm((8, 24, KEYS), BF16),
        "s3": vm((8, 32, KEYS), BF16), "r3": vm((8, 32, KEYS), BF16),
        "mixed": vm((384, 512), BF16), "pbuf": vm((2, 4, 96, HALF), BF16), "prec": vm((2, 2, 96, HALF), BF16), "hop": vm((2, 2, 48, HALF), BF16),
        "stream": vm((96, D), BF16), "oacc": vm((96, D), F32),
        "sel": vm((256, 96), BF16), "whi": vm((256, 96), BF16), "wlo": vm((256, 96), BF16),
        "wg": vm((2, D, 256), BF16), "wu": vm((2, D, 256), BF16), "wd": vm((2, 256, D), BF16),
        "send0": vm((64, 4, HALF), BF16), "recv0": vm((64, 4, HALF), BF16),
        "send1": vm((64, 4, HALF + 128), BF16), "recv1": vm((64, 4, HALF + 128), BF16), "ret": slab, "bk": slab,
        "xb": vm((512, D), BF16), "hid": vm((128, 512), BF16), "yown": vm((256, D), F32),
        "ypart": vm((256, D), BF16), "yrecv": vm((256, D), BF16), "bb": vm((256, D), BF16),
        "lsem": dma(25), "wsend": dma(4), "wrecv": dma(4), "xsem": dma(3), "rsem": dma(3),
        "dsend": dma(8), "drecv": dma(8), "hsend": dma(4), "hrecv": dma(4), "ssem": dma(2), "srecv": dma(2 * CHUNKS),
        "fsend": dma(CHUNKS), "frecv": dma(CHUNKS), "psend": dma(CHUNKS), "precv": dma(CHUNKS),
        "bsend": dma(1), "brecv": dma(CHUNKS),
    }


class Refs:
    def __init__(self, names, refs):
        self.__dict__.update(zip(names, refs))


def layer_kernel(*refs):
    shapes = scratch_shapes()
    r = Refs(INPUTS + ("out",) + tuple(shapes), refs)
    z, y, c, x = place()
    p = y * 2 + c
    sgn = (1 - 2 * (x % 2)) * (1 - 2 * c)
    friend = dev(z, y, c, (x + sgn + 4) % 4)
    facing = dev(z, y, c, (x - sgn + 4) % 4)

    def rank(dz, t):
        return dev((z + dz) % 8, t // 2, t % 2, x)

    plan = {
        "d": [(r.d1, r.d.at[:, :, 0:128]), (r.d2, r.d.at[:, :, 128:384])],
        "k": [(r.k1, r.k.at[:, 0:128]), (r.k2, r.k.at[:, 128:384])],
        "v": [(r.v1, r.v.at[:, 0:256]), (r.v2, r.v.at[:, 256:512])],
        "q": [(r.q1, r.q.at[:, 0:128]), (r.q2, r.q.at[:, 128:384])],
        "g": [(r.g1, r.g.at[:, 0:256]), (r.g2, r.g.at[:, 256:512]),
              (r.n1, r.gain.at[:, 0:128]), (r.n2, r.gain.at[:, 128:256])],
        "i": [(r.ids, r.idv), (r.gw, r.gwv), (r.pw, r.pwv)],
        "o": [(r.ow1, r.ow.at[pl.ds(0, 256)]), (r.ow2, r.ow.at[pl.ds(256, 256)])],
        "s": [(r.res, r.resv), (r.ng, r.ngv)],
        "w": [(r.eg.at[0], r.wg.at[0]), (r.eu.at[0], r.wu.at[0]), (r.ed.at[0], r.wd.at[0])],
    }
    loads, count = {}, 0
    for name, pairs in plan.items():
        loads[name] = []
        for src, dst in pairs:
            loads[name].append(pltpu.make_async_copy(src, dst, r.lsem.at[count]))
            count += 1

    def load(names):
        for name in names:
            for cp in loads[name]:
                cp.start()

    load("dkv")

    def loaded(names):
        for name in names:
            for cp in loads[name]:
                cp.wait()

    barrier = pltpu.get_barrier_semaphore()

    @pl.loop(1, 64)
    def _(o):
        t = (z * 8 + p + o) % 64
        greet(barrier, dev(t // 8, (t // 2) % 4, t % 2, x))

    for o in range(1, 4):
        greet(barrier, dev(z, y, c, (x + o) % 4))

    row = iota2((BLOCK, BLOCK), 0)
    col = iota2((BLOCK, BLOCK), 1)
    lower, upper = row >= col, row <= col
    tri = tuple(jnp.where(m, 1.0, 0.0).astype(BF16) for m in (lower, upper))
    tri = tuple(jnp.concatenate([t, t, t], axis=1) for t in tri)
    scale = jnp.where(iota2((1, KEYS), 1) < 128, 64.0 ** -0.5, 128.0 ** -0.5)
    lane = iota2((1, 256), 1) % 128 < 64
    zero = jnp.zeros((), BF16)
    SPANS = (slice(0, 128), slice(0, 128), slice(128, 256), slice(256, 384))

    def keys_of(n):
        rows = pl.ds(n * BLOCK, BLOCK)
        k = r.k[rows, :].astype(F32)
        ends = []
        for way in range(2):
            d = r.d[way, rows, :].astype(F32)
            rate = (jnp.minimum(d, 0.0) - jnp.log1p(jnp.exp(-jnp.abs(d)))) * (1.0 / 16.0)
            hi = rate.astype(BF16)
            rest = rate - hi.astype(F32)
            mid = rest.astype(BF16)
            low = (rest - mid.astype(F32)).astype(BF16)
            cum = nn(tri[way], jnp.concatenate([hi, mid, low], axis=0))
            r.cum[way, rows, :] = cum
            fade = jnp.exp(cum[BLOCK - 1 :, :] if way == 0 else cum[0:1, :])
            kd = k * jnp.exp(-cum)
            r.kd[way, rows, :] = kd.astype(BF16)
            r.dec[way, n] = jnp.broadcast_to(fade, (8, KEYS))
            ends.append((kd * fade).astype(BF16))
        both = []
        for h, at in enumerate(SPANS):
            v = r.v[rows, 128 * h : 128 * h + 128]
            both.append(tn(v, jnp.concatenate([ends[0][:, at], ends[1][:, at]], axis=1)))
        both[0:2] = [jnp.where(lane, both[0], both[1])]
        for way in range(2):
            for i, b in enumerate(both):
                r.add[way, n, :, 128 * i : 128 * i + 128] = b[:, 128 * way : 128 * way + 128]

    loaded("dkv")
    load("q")
    for n in range(NB):
        keys_of(n)

    pl.semaphore_wait(barrier, 66)
    weights = [
        remote(src, dst, r.wsend.at[i], r.wrecv.at[i], friend)
        for i, (src, dst) in enumerate((
            (r.eg.at[0], r.wg.at[1]),
            (r.eu.at[0, pl.ds(0, HALF)], r.wu.at[1, pl.ds(0, HALF)]),
            (r.eu.at[0, pl.ds(HALF, HALF)], r.wu.at[1, pl.ds(HALF, HALF)]),
            (r.ed.at[0], r.wd.at[1]),
        ))
    ]
    weights[0].start()
    weights[1].start()

    totals, fades = [], []
    for way in range(2):
        order = range(NB) if way == 0 else range(NB - 1, -1, -1)
        run, fade = None, None
        for n in order:
            f = r.dec[way, n][0:1]
            run = r.add[way, n] if run is None else run * f + r.add[way, n]
            fade = f if fade is None else fade * f
        totals.append(run.astype(BF16))
        fades.append(fade)
    tile = jnp.concatenate([t.astype(F32) for f in fades for t in halves(f)] * 2, axis=0).astype(BF16)
    for j in range(8):
        r.s1[j, 0:16, :] = totals[0][16 * j : 16 * j + 16]
        r.s1[j, 16:32, :] = totals[1][16 * j : 16 * j + 16]
        r.s1[j, 32:40, :] = tile
    r.r1[p] = r.s1[p]

    def plane_copy(src, dst, i, o):
        t = (p + o) % 8
        return remote(src.at[t], dst.at[p], r.xsem.at[i], r.rsem.at[i], rank(0, t))

    for o in (4, 3, 5, 2, 6, 1, 7):
        plane_copy(r.s1, r.r1, 0, o).start()

    load("giosw")

    def queries_of(n):
        rows = pl.ds(n * BLOCK, BLOCK)
        q = r.q[rows, :].astype(F32) * scale
        for way in range(2):
            r.qd[way, rows, :] = (q * jnp.exp(r.cum[way, rows, :])).astype(BF16)

    def inner(n):
        rows = pl.ds(n * BLOCK, BLOCK)
        for h, at in enumerate(SPANS):
            m = None if h > 1 else lane[:, 0:128] if h == 0 else jnp.logical_not(lane[:, 0:128])
            s = []
            for way in range(2):
                qd = r.qd[way, rows, at]
                s.append(nt(qd if m is None else jnp.where(m, qd, zero), r.kd[way, rows, at]))
            s = jnp.where(lower, s[0], 0.0) + jnp.where(upper, s[1], 0.0)
            head = slice(128 * h, 128 * h + 128)
            r.acc[rows, head] = nn(s.astype(BF16), r.v[rows, head])

    loaded("q")
    for n in range(NB):
        queries_of(n)
    for n in range(3):
        inner(n)

    def seven(src, dst, i):
        return remote(src.at[pl.ds(0, 7)], dst.at[pl.ds(0, 7)], r.xsem.at[i], r.rsem.at[i], facing)

    batches = [seven(r.s1, r.r1, 0), seven(r.r2, r.r2, 1), seven(r.s3, r.r3, 2)]
    batches[0].wait_recv()

    def unpack(i):
        s = r.r1[i].astype(F32)
        return s[0:16], s[16:32], s[32:33] + s[33:34], s[34:35] + s[35:36]

    parts = [unpack(i) for i in range(8)]
    for way in range(2):
        run, fade = jnp.zeros((16, KEYS), F32), jnp.ones((1, KEYS), F32)
        for i in range(8) if way == 0 else range(7, -1, -1):
            r.pre[way, i] = run
            r.prd[way, i] = jnp.broadcast_to(fade, (8, KEYS))
            run = run * parts[i][2 + way] + parts[i][way]
            fade = fade * parts[i][2 + way]
        hi, lo = halves(fade)
        r.s2[way, 0:16, :] = run.astype(BF16)
        r.s2[way, 16:24, :] = jnp.concatenate([hi.astype(F32), lo.astype(F32)] * 4, axis=0).astype(BF16)
    r.r2[z] = r.s2[0]
    for o in (4, 3, 5, 2, 6, 1, 7):
        remote(r.s2.at[(z + o) // 8], r.r2.at[z], r.xsem.at[1], r.rsem.at[1], rank(o, p)).start()

    for n in range(3, NB):
        inner(n)

    loaded("i")

    def mine(ref):
        pick = ref[:, 288:384]
        for i in (2, 1, 0):
            pick = jnp.where(x == i, ref[:, 96 * i : 96 * i + 96], pick)
        return pick

    ids, gate, pair = mine(r.idv), mine(r.gwv[...][None]), mine(r.pwv)
    inv = gate / (pair[0:1] + pair[1:2])
    experts = iota2((64, 96), 0)
    named = [jnp.where(ids[k : k + 1] == experts, 1.0, 0.0) for k in range(2)]
    before = jnp.where(iota2((96, 96), 0) < iota2((96, 96), 1), 1.0, 0.0).astype(BF16)
    count = nn((named[0] + named[1]).astype(BF16), before)
    slots = [
        jnp.sum(count * named[k], axis=0, keepdims=True).astype(jnp.int32) + 4 * ids[k : k + 1] for k in range(2)
    ]
    for i, dz in enumerate(ORDER):
        here = iota2((32, 96), 0) + 32 * ((z + dz) % 8)
        hits = [jnp.where(slots[k] == here, 1.0, 0.0) for k in range(2)]
        at = slice(32 * i, 32 * i + 32)
        r.sel[at, :] = (hits[0] + hits[1]).astype(BF16)
        r.whi[at, :], r.wlo[at, :] = halves(hits[0] * (inv * pair[0:1]) + hits[1] * (inv * pair[1:2]))

    batches[1].wait_recv()
    entry = []
    for way in range(2):
        run = jnp.zeros((16, KEYS), F32)
        for i in range(8) if way == 0 else range(7, -1, -1):
            s = r.r2[i].astype(F32)
            run = jnp.where(i < z if way == 0 else i > z, run * (s[16:17] + s[17:18]) + s[0:16], run)
        entry.append(run)
    for j in range(8):
        for way in range(2):
            r.s3[j, 16 * way : 16 * way + 16, :] = (
                r.pre[way, j] + r.prd[way, j][0:1] * entry[way]
            ).astype(BF16)
    r.r3[p] = r.s3[p]
    for o in (4, 3, 5, 2, 6, 1, 7):
        plane_copy(r.s3, r.r3, 2, o).start()

    loaded("g")
    for n in range(NB):
        rows = pl.ds(n * BLOCK, BLOCK)
        g = r.g[rows, :].astype(F32)
        gain = r.gain[...]
        gain = jnp.concatenate([gain[:, 0:128], gain[:, 0:128], gain[:, 128:256], gain[:, 128:256]], axis=1)
        r.gs[rows, :] = gain * (g / (1.0 + jnp.exp(-g)))

    batches[2].wait_recv()
    for way in range(2):
        state = jnp.concatenate([r.r3[j, 16 * way : 16 * way + 16, :] for j in range(8)], axis=0).astype(F32)
        for n in range(NB) if way == 0 else range(NB - 1, -1, -1):
            r.st[way, n] = state.astype(BF16)
            state = state * r.dec[way, n][0:1] + r.add[way, n]

    def read_out(n):
        rows = pl.ds(pl.multiple_of(n * BLOCK, BLOCK), BLOCK)
        for h, at in enumerate(SPANS):
            qd = jnp.concatenate([r.qd[0, rows, at], r.qd[1, rows, at]], axis=1)
            if h < 2:
                qd = jnp.where(lane if h == 0 else jnp.logical_not(lane), qd, zero)
            head = slice(128 * h, 128 * h + 128)
            t = r.acc[rows, head] + nt(qd, jnp.concatenate([r.st[0, n, :, at], r.st[1, n, :, at]], axis=1))
            t = t * lax.rsqrt(jnp.mean(t * t, axis=1, keepdims=True) + EPS)
            r.mixed[rows, head] = (t * r.gs[rows, head]).astype(BF16)

    def beside(side):
        return dev(z, y, c, (x + 1 + 2 * side) % 4)

    def band(i):
        return pl.ds(pl.multiple_of(48 * i, 16), 48)

    def hop_copy(cs, side):
        i = 2 * cs + side
        return remote(r.pbuf.at[cs, 3, band(side)], r.hop.at[cs, side], r.hsend.at[i], r.hrecv.at[i], beside(side))

    def owner_copy(cs, side, merged):
        rows = band(side if merged else 1 - side)
        i = 4 * cs + 2 * side + (1 if merged else 0)
        return remote(r.pbuf.at[cs, 1 + side, rows], r.prec.at[cs, side, rows], r.dsend.at[i], r.drecv.at[i], beside(side))

    def project(t, slot, cs):
        rows = r.mixed[pl.ds(pl.multiple_of(t * 96, 32), 96), :]
        for q in range(2):
            at = slice(512 * q, 512 * q + 512)
            r.pbuf[cs, slot, :, at] = nn(rows, r.ow[:, HALF * cs + 512 * q : HALF * cs + 512 * q + 512]).astype(BF16)

    def to_neighbour(side, cs):
        project((x + 1 + 2 * side) % 4, 1 + side, cs)
        owner_copy(cs, side, False).start()

    def merge(cs, side):
        hop_copy(cs, side).wait_recv()
        rows = band(side)
        for q in range(2):
            at = slice(512 * q, 512 * q + 512)
            both = r.pbuf[cs, 1 + side, rows, at].astype(F32) + r.hop[cs, side, :, at].astype(F32)
            r.pbuf[cs, 1 + side, rows, at] = both.astype(BF16)
        owner_copy(cs, side, True).start()

    def own_rows(cs):
        for side in range(2):
            for merged in (False, True):
                owner_copy(cs, side, merged).wait_recv()
        for q in range(2):
            at = slice(512 * q, 512 * q + 512)
            wide = slice(HALF * cs + 512 * q, HALF * cs + 512 * q + 512)
            total = r.pbuf[cs, 0, :, at].astype(F32)
            for side in range(2):
                total = total + r.prec[cs, side, :, at].astype(F32)
            r.stream[:, wide] = (r.resv[:, wide].astype(F32) + total.astype(BF16).astype(F32)).astype(BF16)

    across = (x + 2) % 4
    half = across // 2
    near = 1 - x % 2
    far = 1 - near
    odd = across % 2
    read_out(3 * half + odd)
    read_out(3 * half + odd + 1)
    loaded("o")
    project(across, 3, 0)
    hop_copy(0, 0).start()
    hop_copy(0, 1).start()
    read_out(3 * half + 2 - 2 * odd)
    for i in range(3):
        read_out(3 * (1 - half) + i)
    to_neighbour(near, 0)
    to_neighbour(far, 0)
    project(across, 3, 1)
    hop_copy(1, 0).start()
    hop_copy(1, 1).start()
    merge(0, near)
    merge(0, far)
    to_neighbour(near, 1)
    to_neighbour(far, 1)
    project(x, 0, 0)
    project(x, 0, 1)
    merge(1, near)
    merge(1, far)
    weights[2].start()
    weights[3].start()
    loaded("s")

    def scatter_rows(dst, first, rows, at):
        for e in range(rows.shape[0] // 4):
            dst[first + e, :, at] = rows[4 * e : 4 * e + 4, :]

    def slabs_out(src, dst, ssem, rsem, *groups):
        for i in groups:
            @pl.loop(1 if ORDER[i] == 0 else 0, 8)
            def _(o):
                t = (p + o) % 8
                remote(src.at[i * 8 + t], dst.at[MIRROR[i] * 8 + p], ssem, rsem, rank(ORDER[i], t)).start()

    def slabs_in(src, dst, ssem, rsem, k):
        n = 15 if k == 0 else 16
        return remote(src.at[pl.ds(0, n)], dst.at[pl.ds(0, n)], ssem, rsem, facing)

    sides = ((r.send0, r.recv0), (r.send1, r.recv1))

    def fill(cs, k):
        span = slice(64 * k, 64 * k + 64)
        for q in range(2):
            at = slice(512 * q, 512 * q + 512)
            rows = nn(r.sel[span, :], r.stream[:, HALF * cs + 512 * q : HALF * cs + 512 * q + 512])
            scatter_rows(sides[cs][0], 16 * k, rows.astype(BF16), at)
        if cs:
            scatter_rows(r.send1, 16 * k, nn(r.sel[span, :], scales).astype(BF16), slice(HALF, HALF + 128))
        if k == 0:
            sides[cs][1][8 + p] = sides[cs][0][8 + p]

    def dispatch(cs, k):
        slabs_out(*sides[cs], r.ssem.at[cs], r.srecv.at[4 * cs + k], 2 * k, 2 * k + 1)

    own_rows(0)
    fill(0, 0)
    dispatch(0, 0)
    fill(0, 1)
    dispatch(0, 1)
    fill(0, 2)
    fill(0, 3)
    own_rows(1)
    wide = r.stream[...].astype(F32)
    inv_rms = lax.rsqrt(jnp.mean(wide * wide, axis=1, keepdims=True) + EPS)
    hi = inv_rms.astype(BF16).astype(F32)
    mid = (inv_rms - hi).astype(BF16).astype(F32)
    low = inv_rms - hi - mid
    which = iota2((96, 128), 1)
    scales = jnp.where(which == 0, hi, jnp.where(which == 1, mid, jnp.where(which == 2, low, 0.0))).astype(BF16)
    fill(1, 0)
    dispatch(1, 0)
    fill(1, 1)
    dispatch(1, 1)
    dispatch(0, 2)
    dispatch(0, 3)
    fill(1, 2)
    dispatch(1, 2)
    fill(1, 3)
    dispatch(1, 3)
    r.oacc[...] = wide

    def forward(k):
        return remote(
            r.xb.at[pl.ds(128 * k, 64)], r.xb.at[pl.ds(128 * k + 64, 64)], r.fsend.at[k], r.frecv.at[k], facing
        )

    def partial(k):
        span = pl.ds(64 * k, 64)
        return remote(r.ypart.at[span], r.yrecv.at[span], r.psend.at[k], r.precv.at[k], facing)

    def arrive(k):
        for cs in range(2):
            slabs_in(*sides[cs], r.ssem.at[cs], r.srecv.at[4 * cs + k], k).wait_recv()
        for i in range(2):
            rows = slice(128 * k + 32 * i, 128 * k + 32 * i + 32)
            first, last = (
                jnp.concatenate([ref[16 * k + 8 * i + j] for j in range(8)], axis=0).astype(F32)
                for ref in (r.recv0, r.recv1)
            )
            inv_rms = jnp.sum(last[:, HALF:], axis=1, keepdims=True)
            r.xb[rows, 0:HALF] = (first * inv_rms * r.ngv[:, 0:HALF]).astype(BF16)
            r.xb[rows, HALF:D] = (last[:, 0:HALF] * inv_rms * r.ngv[:, HALF:D]).astype(BF16)
        forward(k).start()

    def experts_on(k):
        if k == 0:
            loaded("w")
            for cp in weights[0:3]:
                cp.wait_recv()
        forward(k).wait_recv()
        rows = pl.ds(128 * k, 128)
        for s in range(2):
            a = nn(r.xb[rows, :], r.wg[s])
            b = nn(r.xb[rows, :], r.wu[s])
            r.hid[:, 256 * s : 256 * s + 256] = (a / (1.0 + jnp.exp(-a)) * b).astype(BF16)
        if k == 0:
            weights[3].wait_recv()
        for q in range(4):
            at = slice(512 * q, 512 * q + 512)
            out = nn(r.hid[:, 0:256], r.wd[0, :, at]) + nn(r.hid[:, 256:512], r.wd[1, :, at])
            r.yown[64 * k : 64 * k + 64, at] = out[0:64]
            r.ypart[64 * k : 64 * k + 64, at] = out[64:128].astype(BF16)
        partial(k).start()

    def give_back(k):
        partial(k).wait_recv()
        for i in (2 * k, 2 * k + 1):
            span = slice(32 * i, 32 * i + 32)
            for q in range(4):
                at = slice(512 * q, 512 * q + 512)
                rows = r.yown[span, at] + r.yrecv[span, at].astype(F32)
                scatter_rows(r.ret, 8 * i, rows.astype(BF16), at)
            if ORDER[i] == 0:
                r.bk[8 * i + p] = r.ret[8 * i + p]
            slabs_out(r.ret, r.bk, r.bsend.at[0], r.brecv.at[k], i)

    arrive(0)
    arrive(1)
    experts_on(0)
    experts_on(1)
    give_back(0)
    arrive(2)
    arrive(3)
    give_back(1)
    experts_on(2)
    experts_on(3)
    give_back(2)
    give_back(3)

    def gather_back(k):
        slabs_in(r.ret, r.bk, r.bsend.at[0], r.brecv.at[k], k).wait_recv()
        for i in range(2):
            r.bb[64 * k + 32 * i : 64 * k + 32 * i + 32, :] = jnp.concatenate(
                [r.bk[16 * k + 8 * i + j] for j in range(8)], axis=0
            )

    for k in range(CHUNKS):
        gather_back(k)
        span = slice(64 * k, 64 * k + 64)
        for q in range(4):
            at = slice(512 * q, 512 * q + 512)
            total = r.oacc[:, at] + tn(r.whi[span, :], r.bb[span, at]) + tn(r.wlo[span, :], r.bb[span, at])
            if k < CHUNKS - 1:
                r.oacc[:, at] = total
            else:
                r.out[:, at] = total.astype(BF16)

    for batch in batches:
        batch.wait_send()
    for cs in range(2):
        for side in range(2):
            hop_copy(cs, side).wait_send()
            for merged in (False, True):
                owner_copy(cs, side, merged).wait_send()
    for cp in weights:
        cp.wait_send()
    for src, dst, ssem, rsem in (
        (r.send0, r.recv0, r.ssem.at[0], r.srecv.at[0]),
        (r.send1, r.recv1, r.ssem.at[1], r.srecv.at[4]),
        (r.ret, r.bk, r.bsend.at[0], r.brecv.at[0]),
    ):
        remote(src.at[pl.ds(0, 63)], dst.at[pl.ds(0, 63)], ssem, rsem, facing).wait_send()
    for k in range(CHUNKS):
        forward(k).wait_send()
        partial(k).wait_send()


def body(
    residual, query_one, key_one, value_one, gate_one, decay_one, norm_one, output_one,
    query_two, key_two, value_two, gate_two, decay_two, norm_two, output_two, norm_gain,
    expert_ids, group_weight, pair_weight, expert_gate, expert_up, expert_down,
):
    return pl.pallas_call(
        layer_kernel,
        name="layer",
        out_shape=jax.ShapeDtypeStruct((96, D), BF16),
        in_specs=[pl.BlockSpec(memory_space=pltpu.HBM)] * len(INPUTS),
        out_specs=pl.BlockSpec(memory_space=pltpu.VMEM),
        scratch_shapes=list(scratch_shapes().values()),
        compiler_params=pltpu.CompilerParams(
            collective_id=0, has_side_effects=True, vmem_limit_bytes=60 * 1024 * 1024
        ),
    )(
        residual, query_one, key_one, value_one, gate_one, decay_one, norm_one[None], output_one,
        query_two, key_two, value_two, gate_two, decay_two, norm_two[None], output_two, norm_gain[None],
        expert_ids.T, group_weight, pair_weight.T, expert_gate, expert_up, expert_down,
    )


def solution(mesh):
    torus = Mesh(mesh.devices.reshape(8, 4, 2, mesh.shape["tp"]), SP_TP)
    heads = P(SP, "tp")
    in_specs = (
        P(SP_TP, None), heads, heads, heads, heads, P(None, SP, "tp"), P(), P("tp", None),
        heads, heads, heads, heads, P(None, SP, "tp"), P(), P("tp", None),
        P(), P(SP, None), P(SP), P(SP, None), P(SP, None, "tp"), P(SP, None, "tp"), P(SP, "tp", None),
    )
    return jax.shard_map(body, mesh=torus, in_specs=in_specs, out_specs=P(SP_TP, None), check_vma=False)
```
